32 devices in a mesh: grp: 2 (over y), sp: 4 (over z), tp: 4 (over x, core).
Axes of the slice: x: 2, y: 2, z: 4, core: 2. Of those that a mesh axis runs over, the one named last changes fastest.
Arguments:
- hidden_in: bfloat16 [2048, 2048], P(('grp', 'sp')), parts along dimension 0, may hold values from -6 to 6
- query_latent_rows: bfloat16 [2048, 768], P(('grp', 'sp')), parts along dimension 0, may hold values from -6 to 6
- key_value_latent: bfloat16 [2048, 512], P(('grp', 'sp')), parts along dimension 0, may hold values from -6 to 6
- rotary_key: bfloat16 [2048, 32], P(('grp', 'sp')), parts along dimension 0, may hold values from -64 to 64
- query_norm_gain: float32 [768], replicated, may hold values from 0.1 to 1.9
- key_value_gain: float32 [512], replicated, may hold values from 0.1 to 1.9
- query_up_weight: bfloat16 [768, 1536], P(None, 'tp'), may hold values from -0.625 to 0.625
- key_value_up_weight: bfloat16 [512, 2048], P(None, 'tp'), may hold values from -0.25 to 0.25
- out_proj: bfloat16 [1024, 2048], P('tp'), may hold values from -0.1875 to 0.1875
- feed_gain: float32 [2048], replicated, may hold values from 0.1 to 1.9
- feed_up: bfloat16 [2048, 8192], P('sp', 'tp'), may hold values from -0.125 to 0.125
- feed_down: bfloat16 [8192, 2048], P('tp', 'sp'), may hold values from -0.0625 to 0.0625
Outputs:
- layer_out: bfloat16 [2048, 2048], P(('grp', 'sp', 'tp')), parts along dimension 0
The draws below stay inside these ranges and needn't reach their ends.
There are 2 independent parts, one for each index of `grp`. The reference program is written for one: setup_inputs(seed, part) draws one part's arguments, and reference() takes and returns one part's arrays. A program takes and returns all parts, laid end to end along the dimension named above; an argument that names none is the same for every part. Nothing has to cross between parts.
All inputs are finite; a program needn't handle non-finite values.
Results may differ from the reference program's by a relative error of at most 0.02.
Values may be sent and summed in bfloat16 or wider, within the bound.
A program may use at most 128 MiB of HBM per device.

```python
import math
import jax
import jax.numpy as jnp
from jax import lax

D = 2048
HEAD_COUNT = 16
QUERY_KEY_PLAIN = 64
QUERY_KEY_ROTARY = 32
VALUE_HEAD_SIZE = 64
QUERY_RANK = 768
KEY_VALUE_RANK = 512
FF = 8192
TOKEN_COUNT = 1024


def draw_rotary_key(key, part):
    base = jax.random.normal(jax.random.fold_in(key, 11), (TOKEN_COUNT, QUERY_KEY_ROTARY), jnp.float32)
    return jnp.clip(base, -64.0, 64.0).astype(jnp.bfloat16)


def levels(stream_key, shape, shards, smallest, largest):
    level = 1.0
    for axis_at, blocks in shards:
        heights = jax.random.uniform(jax.random.fold_in(jax.random.fold_in(stream_key, 6), axis_at), (blocks,), jnp.float32, smallest / len(shards), largest / len(shards))
        level = level * jnp.repeat(jnp.exp(heights), shape[axis_at] // blocks).reshape((-1,) + (1,) * (len(shape) - 1 - axis_at))
    return level


def centred(stream_key, extent, deviation, limit, shards=(), kind=jnp.bfloat16):
    factor_of = levels(stream_key, extent, shards, -0.22, 0.18) if shards else 1.0
    drawn = jax.random.normal(stream_key, extent, jnp.float32) * deviation * factor_of
    return jnp.minimum(jnp.maximum(drawn, -limit), limit).astype(kind)


def setup_inputs(seed: int = 0, part: int = 0) -> dict:
    streams_of = jax.random.split(jax.random.key(seed), 13)
    part_keys = jax.random.split(jax.random.fold_in(streams_of[12], part), 13)
    hidden_in = centred(part_keys[0], (TOKEN_COUNT, D), 1.0, 6.0, ((0, 4),))
    query_latent_rows = centred(part_keys[1], (TOKEN_COUNT, QUERY_RANK), 1.0, 6.0, ((0, 4),))
    key_value_latent = centred(part_keys[2], (TOKEN_COUNT, KEY_VALUE_RANK), 1.0, 6.0, ((0, 4),))
    rotary_key = draw_rotary_key(jax.random.fold_in(jax.random.fold_in(streams_of[12], part), 71), part)
    query_norm_gain = jnp.clip(1.0 + 0.18 * jax.random.normal(streams_of[4], (QUERY_RANK,), jnp.float32), 0.1, 1.9)
    key_value_gain = jnp.clip(1.0 + 0.18 * jax.random.normal(streams_of[5], (KEY_VALUE_RANK,), jnp.float32), 0.1, 1.9)
    query_up_weight = centred(streams_of[6], (QUERY_RANK, HEAD_COUNT * (QUERY_KEY_PLAIN + QUERY_KEY_ROTARY)), (3 * QUERY_RANK ** -0.5), 0.625, ((1, 4),))
    key_value_up_weight = centred(streams_of[7], (KEY_VALUE_RANK, HEAD_COUNT * (QUERY_KEY_PLAIN + VALUE_HEAD_SIZE)), KEY_VALUE_RANK ** -0.5, 0.25, ((1, 4),))
    out_proj = centred(streams_of[8], (HEAD_COUNT * VALUE_HEAD_SIZE, D), (HEAD_COUNT * VALUE_HEAD_SIZE) ** -0.5, 0.1875, ((0, 4),))
    feed_gain = jnp.clip(1.0 + 0.18 * jax.random.normal(streams_of[9], (D,), jnp.float32), 0.1, 1.9)
    feed_up = centred(streams_of[10], (D, FF), D ** -0.5, 0.125, ((0, 4), (1, 4)))
    feed_down = centred(streams_of[11], (FF, D), FF ** -0.5, 0.0625, ((0, 4), (1, 4)))
    return {"hidden_in": hidden_in, "query_latent_rows": query_latent_rows, "key_value_latent": key_value_latent, "rotary_key": rotary_key, "query_norm_gain": query_norm_gain, "key_value_gain": key_value_gain, "query_up_weight": query_up_weight, "key_value_up_weight": key_value_up_weight, "out_proj": out_proj, "feed_gain": feed_gain, "feed_up": feed_up, "feed_down": feed_down}


def normalize(values, gain):
    floats = values.astype(jnp.float32)
    return floats * lax.rsqrt(lax.optimization_barrier(jnp.mean(floats * floats, axis=-1, keepdims=True)) + 1e-06) * gain.astype(jnp.float32)

def rotate(values, position):
    half_size = values.shape[-1] // 2
    inverse = 10000.0 ** (-jnp.arange(half_size, dtype=jnp.float32) * 2.0 / values.shape[-1])
    angles = position[:, None] * inverse[None, :]
    cosine = jnp.concatenate([jnp.cos(angles), jnp.cos(angles)], axis=-1)
    sine = jnp.concatenate([jnp.sin(angles), jnp.sin(angles)], axis=-1)
    shape = (values.shape[0],) + (1,) * (values.ndim - 2) + (values.shape[-1],)
    turned = jnp.concatenate([-values[..., half_size:], values[..., :half_size]], axis=-1)
    return values * cosine.reshape(shape) + turned * sine.reshape(shape)

def reference(hidden_in, query_latent_rows, key_value_latent, rotary_key, query_norm_gain, key_value_gain, query_up_weight, key_value_up_weight, out_proj, feed_gain, feed_up, feed_down):
    position = jnp.arange(TOKEN_COUNT).astype(jnp.float32)
    scale_factor = (QUERY_KEY_PLAIN + QUERY_KEY_ROTARY) ** (-0.5)
    query_norm = normalize(query_latent_rows, query_norm_gain).astype(jnp.bfloat16)
    queries = jnp.dot(query_norm, query_up_weight, preferred_element_type=jnp.float32).reshape(TOKEN_COUNT, HEAD_COUNT, QUERY_KEY_PLAIN + QUERY_KEY_ROTARY)
    queries = jnp.concatenate([queries[..., :QUERY_KEY_PLAIN], rotate(queries[..., QUERY_KEY_PLAIN:], position)], axis=-1).astype(jnp.bfloat16)
    latent = normalize(key_value_latent, key_value_gain).astype(jnp.bfloat16)
    keys_values = jnp.dot(latent, key_value_up_weight, preferred_element_type=jnp.float32).astype(jnp.bfloat16)
    keys_values = keys_values.reshape(TOKEN_COUNT, HEAD_COUNT, QUERY_KEY_PLAIN + VALUE_HEAD_SIZE)
    key_nope = keys_values[..., :QUERY_KEY_PLAIN].astype(jnp.float32)
    value_rows = keys_values[..., QUERY_KEY_PLAIN:].astype(jnp.float32)
    key_rope = rotate(rotary_key.astype(jnp.float32), position).astype(jnp.bfloat16).astype(jnp.float32)
    block = math.gcd(TOKEN_COUNT, 512)
    query_blocks = queries.reshape(TOKEN_COUNT // block, block, HEAD_COUNT, QUERY_KEY_PLAIN + QUERY_KEY_ROTARY)

    def attend(query_block):
        plain = query_block[..., :QUERY_KEY_PLAIN].astype(jnp.float32)
        turned = query_block[..., QUERY_KEY_PLAIN:].astype(jnp.float32)
        scores = jnp.einsum('qhd,khd->hqk', plain, key_nope) + jnp.einsum('qhd,kd->hqk', turned, key_rope)
        scores = scores * scale_factor
        expo = jnp.exp(scores - lax.optimization_barrier(jnp.max(scores, axis=-1, keepdims=True)))
        total = lax.optimization_barrier(jnp.sum(expo, axis=-1))
        weights = expo.astype(jnp.bfloat16).astype(jnp.float32)
        summed = jnp.einsum('hqk,khd->qhd', weights, value_rows)
        return summed / jnp.transpose(total)[:, :, None]
    mixed = lax.map(attend, query_blocks).reshape(TOKEN_COUNT, HEAD_COUNT * VALUE_HEAD_SIZE).astype(jnp.bfloat16)
    branch = jnp.dot(mixed, out_proj, preferred_element_type=jnp.float32)
    middle = (hidden_in.astype(jnp.float32) + branch).astype(jnp.bfloat16)
    normed = normalize(middle, feed_gain).astype(jnp.bfloat16)
    upward = jnp.dot(normed, feed_up, preferred_element_type=jnp.float32)
    activated = jnp.square(jax.nn.relu(upward)).astype(jnp.bfloat16)
    feed = jnp.dot(activated, feed_down, preferred_element_type=jnp.float32)
    return (middle.astype(jnp.float32) + feed).astype(jnp.bfloat16)
```

```python
import math

import jax
import jax.numpy as jnp
import numpy as np
from jax import lax
from jax.experimental import pallas as pl
from jax.experimental.pallas import tpu as pltpu
from jax.sharding import PartitionSpec as P

QUERY_KEY_PLAIN = 64
QUERY_KEY_ROTARY = 32
VALUE_HEAD_SIZE = 64


def normalize(values, gain):
    floats = values.astype(jnp.float32)
    return floats * lax.rsqrt(jnp.mean(floats * floats, axis=-1, keepdims=True) + 1e-06) * gain


def rotate(values, position):
    half_size = values.shape[-1] // 2
    inverse = 10000.0 ** (-jnp.arange(half_size, dtype=jnp.float32) * 2.0 / values.shape[-1])
    angles = position[:, None] * inverse[None, :]
    cosine = jnp.concatenate([jnp.cos(angles), jnp.cos(angles)], axis=-1)
    sine = jnp.concatenate([jnp.sin(angles), jnp.sin(angles)], axis=-1)
    shape = (values.shape[0],) + (1,) * (values.ndim - 2) + (values.shape[-1],)
    turned = jnp.concatenate([-values[..., half_size:], values[..., :half_size]], axis=-1)
    return values * cosine.reshape(shape) + turned * sine.reshape(shape)


MESH = pl.DeviceIdType.MESH


def layer_kernel(
    n, heads, table, kvlat, rk, qlat, gq, gkv, gain, turn, perm, wq, wkv, hidden, op, up, down, out,
    lat_in, rk_in, q_in, wq_in, wkv_in, perm_in, hid_in,
    lat_all, kv_all, q_all, op_all, mixed, mixed_in, up_all, down_all, middle, norm_all, act, part,
    rf1, c2, rf2, c3, rf3, ss, rs, ls,
):
    g, me, t = lax.axis_index("grp"), lax.axis_index("sp"), lax.axis_index("tp")
    c, x = lax.rem(t, 2), t // 2
    share, width = middle.shape
    rows = share * 4
    rank = wkv.shape[0]
    piece_k = up.shape[0]
    hid = down_all.shape[0]
    half_k, half_h = piece_k // 2, hid // 2
    wide = down.shape[1]
    bf, f32 = jnp.bfloat16, jnp.float32
    vh = VALUE_HEAD_SIZE
    unit = QUERY_KEY_PLAIN + vh
    lanes = heads * QUERY_KEY_ROTARY
    scale_factor = (QUERY_KEY_PLAIN + QUERY_KEY_ROTARY) ** (-0.5)
    inner = jnp.minimum(me, n - 1 - me)

    def near(i):
        if i == 0:
            return me
        step = (i + 1) // 2
        turned = me - step if i % 2 else me + step
        return jnp.where(i <= 2 * inner, turned, jnp.where(2 * me < n - 1, i, n - 1 - i))

    def at_tp(cc, xx):
        return {"tp": xx * 2 + cc}

    sib, xpeer, ypeer = at_tp(1 - c, x), at_tp(c, 1 - x), {"grp": 1 - g}
    barrier = pltpu.get_barrier_semaphore()
    for i in range(1, n):
        pl.semaphore_signal(barrier, inc=1, device_id={"sp": near(i)}, device_id_type=MESH)
    for peer in (sib, xpeer, at_tp(1 - c, 1 - x), ypeer):
        pl.semaphore_signal(barrier, inc=1, device_id=peer, device_id_type=MESH)

    def rows_of(tt):
        return pl.ds(pl.multiple_of(tt * share, share), share)

    mine = rows_of(t)
    local = []

    def fetch(src, dst):
        copy = pltpu.make_async_copy(src, dst, ls.at[len(local)])
        copy.start()
        local.append(copy)
        return copy

    got_lat = fetch(kvlat.at[mine], lat_in)
    got_rk = fetch(rk.at[mine], rk_in)
    got_perm = fetch(perm, perm_in)
    got_wq = fetch(wq, wq_in)
    got_q = fetch(qlat, q_in)
    got_wkv = fetch(wkv, wkv_in)
    op_rows = op.shape[0]
    got_op = fetch(op, op_all.at[pl.ds(pl.multiple_of(t * op_rows, op_rows), op_rows)])
    got_hid = fetch(hidden.at[mine], hid_in)
    got_up = fetch(
        up.at[:, pl.ds(pl.multiple_of(me * hid, hid), hid)],
        up_all.at[pl.ds(pl.multiple_of(me * piece_k, piece_k), piece_k)],
    )
    got_down = fetch(
        down.at[pl.ds(pl.multiple_of(me * hid, hid), hid)],
        down_all.at[:, pl.ds(pl.multiple_of(me * wide, wide), wide)],
    )

    names = {}
    sent = []

    def slot(name, at):
        if name not in names:
            names[name] = sum(size for _, size in names.values()), 1 if at is None else n
        return names[name][0] + (0 if at is None else at)

    def send(name, src, dst, dev, to=None, by=None):
        copy = pltpu.make_async_remote_copy(
            src_ref=src, dst_ref=dst, send_sem=ss.at[slot(name, to)], recv_sem=rs.at[slot(name, by)],
            device_id=dev, device_id_type=MESH,
        )
        copy.start()
        sent.append(copy)

    def land(name, dst, by=None):
        pltpu.make_async_remote_copy(
            src_ref=dst, dst_ref=dst, send_sem=ss.at[slot(name, by)], recv_sem=rs.at[slot(name, by)],
            device_id=sib, device_id_type=MESH,
        ).wait_recv()

    def up_half(owner, hv):
        return up_all.at[pl.ds(pl.multiple_of(owner * piece_k + hv * half_k, half_k), half_k)]

    def down_half(owner, hv):
        return down_all.at[
            pl.ds(pl.multiple_of(hv * half_h, half_h), half_h),
            pl.ds(pl.multiple_of(owner * wide, wide), wide),
        ]

    def begin(tag, buf):
        own = buf.at[me, c, x]
        send((tag, "x"), own, own, xpeer, me, me)
        for i in reversed(range(1, n)):
            send((tag, "z"), own, own, {"sp": near(i)}, near(i), me)
        send((tag, "s"), own, own, sib, me, me)

    def relay(tag, buf, i):
        z = near(i)
        piece = buf.at[z, c, x]
        land((tag, "z"), piece, z)
        send((tag, "x"), piece, piece, xpeer, z, z)
        send((tag, "s"), piece, piece, sib, z, z)

    def cross(tag, buf, i):
        z = near(i)
        piece = buf.at[z, c, 1 - x]
        land((tag, "x"), piece, z)
        send((tag, "t"), piece, piece, sib, z, z)

    def settle(tag, buf, i):
        z = near(i)
        land((tag, "s"), buf.at[z, 1 - c, x], z)
        land((tag, "t"), buf.at[z, 1 - c, 1 - x], z)

    got_lat.wait()
    got_rk.wait()
    lat_all[me, c, x, :, :rank] = normalize(lat_in[...], gkv[...]).astype(bf)
    spun = jnp.dot(rk_in[...], turn[...], preferred_element_type=f32)
    lat_all[me, c, x, :, rank:] = (
        spun[:, :lanes] * table[0, mine, :] + spun[:, lanes:] * table[1, mine, :]
    ).astype(bf)
    pl.semaphore_wait(barrier, n + 3)
    begin("l", lat_all)
    for i in reversed(range(1, n)):
        send(
            "up",
            up.at[
                pl.ds(pl.multiple_of(g * half_k, half_k), half_k),
                pl.ds(pl.multiple_of(near(i) * hid, hid), hid),
            ],
            up_half(me, g),
            {"sp": near(i)},
            near(i),
            me,
        )

    op_parts = 4
    op_piece = op_rows // op_parts

    def op_block(tt, j):
        return op_all.at[pl.ds(pl.multiple_of(tt * op_rows + j * op_piece, op_piece), op_piece)]

    def send_op(j):
        own = op_block(t, j)
        send(("ox", j), own, own, xpeer)

    got_op.wait()
    send_op(0)
    own_op = op_all.at[pl.ds(pl.multiple_of(t * op_rows, op_rows), op_rows)]
    send("os", own_op, own_op, sib)

    got_perm.wait()
    got_wq.wait()
    wide_q = jnp.dot(wq_in[...], perm_in[...], preferred_element_type=f32).astype(bf)
    got_q.wait()
    query_norm = normalize(q_in[...], gq[...]).astype(bf)
    spread = jnp.dot(query_norm, wide_q, preferred_element_type=f32)
    first = heads * unit
    spin = (
        spread[:, first : first + lanes] * table[0] + spread[:, first + lanes : first + 2 * lanes] * table[1]
    )
    lane = lax.broadcasted_iota(jnp.int32, (rows, lanes), 1)
    for h in range(heads):
        q_all[h, :, :unit] = spread[:, h * unit : (h + 1) * unit].astype(bf)
        keep = (lane >= h * QUERY_KEY_ROTARY) & (lane < (h + 1) * QUERY_KEY_ROTARY)
        q_all[h, :, unit:] = jnp.where(keep, spin, 0.0).astype(bf)

    for i in range(1, n):
        relay("l", lat_all, i)
    for j in range(1, op_parts):
        send_op(j)
    got_wkv.wait()
    for i in range(n):
        cross("l", lat_all, i)
    for i in range(n):
        settle("l", lat_all, i)
    for j in range(n):
        made = jnp.dot(
            lat_all[j, :, :, :, :rank].reshape(rows, rank), wkv_in[...], preferred_element_type=f32
        ).astype(bf)
        rope = lat_all[j, :, :, :, rank:].reshape(rows, lanes)
        for h in range(heads):
            kv_all[h, j * rows : (j + 1) * rows, :unit] = made[:, h * unit : (h + 1) * unit]
            kv_all[h, j * rows : (j + 1) * rows, unit:] = rope

    contract = (((1,), (1,)), ((), ()))
    low = lax.broadcasted_iota(jnp.int32, (rows, unit), 1) < vh

    def attend(h):
        scores = lax.dot_general(q_all[h], kv_all[h], contract, preferred_element_type=f32)
        scores = scores * scale_factor
        expo = jnp.exp(scores - jnp.max(scores, axis=-1, keepdims=True))
        total = jnp.sum(expo, axis=-1, keepdims=True)
        mix = jnp.dot(expo.astype(bf), kv_all[h, :, :unit], preferred_element_type=f32)
        return mix / total

    others = ((c, 1 - x), (1 - c, 1 - x), (1 - c, x))
    for p in range(heads // 2):
        left, right = attend(2 * p), attend(2 * p + 1)
        pair = jnp.where(low, pltpu.roll(left, vh, 1), right)
        mixed[p] = pair.astype(bf)
        cols = pl.ds(pl.multiple_of(t * heads * vh + p * unit, unit), unit)
        for j, (cc, xx) in enumerate(others):
            send(
                ("m", p, j), mixed.at[p, rows_of(xx * 2 + cc)], mixed_in.at[:, cols], at_tp(cc, xx)
            )
        mixed_in[:, cols] = mixed[p, mine, :]

    for j in range(op_parts):
        piece = op_block((1 - x) * 2 + c, j)
        land(("ox", j), piece)
        send(("ot", j), piece, piece, sib)
    for i in range(1, n):
        piece = up_half(near(i), g)
        land("up", piece, near(i))
        send("uy", piece, piece, ypeer, near(i), near(i))
    land("os", op_all.at[pl.ds(pl.multiple_of((x * 2 + 1 - c) * op_rows, op_rows), op_rows)])
    for j in range(op_parts):
        land(("ot", j), op_block((1 - x) * 2 + 1 - c, j))
    for p in range(heads // 2):
        for j, (cc, xx) in enumerate(others):
            cols = pl.ds(pl.multiple_of((xx * 2 + cc) * heads * vh + p * unit, unit), unit)
            land(("m", p, j), mixed_in.at[:, cols])

    tile = math.gcd(width, 512)
    got_hid.wait()

    @pl.loop(0, width // tile)
    def _(j):
        cols = pl.ds(pl.multiple_of(j * tile, tile), tile)
        branch = jnp.dot(mixed_in[...], op_all[:, cols], preferred_element_type=f32)
        middle[:, cols] = (hid_in[:, cols].astype(f32) + branch).astype(bf)

    norm_all[me, c, x] = normalize(middle[...], gain[...]).astype(bf)

    begin("n", norm_all)
    for i in reversed(range(1, n)):
        send(
            "dn",
            down.at[pl.ds(pl.multiple_of(near(i) * hid + g * half_h, half_h), half_h)],
            down_half(me, g),
            {"sp": near(i)},
            near(i),
            me,
        )

    def raise_block(i):
        z = near(i)
        upward = jnp.dot(norm_all[z].reshape(rows, width), up_all[...], preferred_element_type=f32)
        act[z] = jnp.square(jnp.maximum(upward, 0.0)).astype(bf)

    for i in range(1, n):
        land("uy", up_half(near(i), 1 - g), near(i))
    got_up.wait()
    relay("n", norm_all, 1)
    for i in range(n):
        cross("n", norm_all, i)
        if i + 2 < n:
            relay("n", norm_all, i + 2)
        settle("n", norm_all, i)
        raise_block(i)
    for i in range(1, n):
        piece = down_half(near(i), g)
        land("dn", piece, near(i))
        send("dy", piece, piece, ypeer, near(i), near(i))
    got_down.wait()
    for i in range(1, n):
        land("dy", down_half(near(i), 1 - g), near(i))

    def lower(i):
        dest = near(i)

        @pl.loop(0, width // tile)
        def _(j):
            cols = pl.ds(pl.multiple_of(j * tile, tile), tile)
            made = jnp.dot(act[dest], down_all[:, cols], preferred_element_type=f32)
            part[i, :, :, :, cols] = made.astype(bf).reshape(2, 2, share, tile)

        send(("f1", i), part.at[i, 1 - c], rf1.at[i], sib)

    def fold_core(i):
        land(("f1", i), rf1.at[i])
        c2[i] = (part[i, c, 1 - x].astype(f32) + rf1[i, 1 - x].astype(f32)).astype(bf)
        send(("f2", i), c2.at[i], rf2.at[i], xpeer)

    def fold_x(i):
        land(("f2", i), rf2.at[i])
        c3[i] = (
            part[i, c, x].astype(f32) + rf1[i, x].astype(f32) + rf2[i].astype(f32)
        ).astype(bf)
        if i:
            send("f3", c3.at[i], rf3.at[me], {"sp": near(i)}, near(i), me)

    order = list(reversed(range(n)))
    for at, i in enumerate(order):
        lower(i)
        if at:
            fold_core(order[at - 1])
    fold_core(order[-1])
    for i in order:
        fold_x(i)
    feed = c3[0].astype(f32)
    for i in range(1, n):
        land("f3", rf3.at[near(i)], near(i))
        feed += rf3[near(i)].astype(f32)
    out[...] = (middle[...].astype(f32) + feed).astype(bf)
    for copy in sent:
        copy.wait_send()


def spread_columns(heads):
    head = QUERY_KEY_PLAIN + QUERY_KEY_ROTARY
    half = QUERY_KEY_ROTARY // 2
    unit = QUERY_KEY_PLAIN + VALUE_HEAD_SIZE
    lanes = heads * QUERY_KEY_ROTARY
    perm = np.zeros((heads * head, heads * unit + 2 * lanes), np.float32)
    turn = np.zeros((QUERY_KEY_ROTARY, 2 * lanes), np.float32)
    for h in range(heads):
        for r in range(QUERY_KEY_PLAIN):
            perm[h * head + r, h * unit + r] = 1.0
        for r in range(QUERY_KEY_ROTARY):
            col = h * QUERY_KEY_ROTARY + r
            other, sign = (r + half, -1.0) if r < half else (r - half, 1.0)
            turn[r, col] = 1.0
            turn[other, lanes + col] = sign
            perm[h * head + QUERY_KEY_PLAIN + r, heads * unit + col] = 1.0
            perm[h * head + QUERY_KEY_PLAIN + other, heads * unit + lanes + col] = sign
    return jnp.asarray(perm, jnp.bfloat16), jnp.asarray(turn, jnp.bfloat16)


def run_layer(
    hidden_in, query_latent_rows, key_value_latent, rotary_key, query_norm_gain, key_value_gain,
    query_up_weight, key_value_up_weight, out_proj, feed_gain, feed_up, feed_down, position,
):
    n = lax.axis_size("sp")
    rows, width = hidden_in.shape
    heads = query_up_weight.shape[1] // (QUERY_KEY_PLAIN + QUERY_KEY_ROTARY)
    share = rows // lax.axis_size("tp")
    hid = feed_up.shape[1] // n
    unit = QUERY_KEY_PLAIN + VALUE_HEAD_SIZE
    lanes = heads * QUERY_KEY_ROTARY
    rank = key_value_latent.shape[1]
    bf = jnp.bfloat16
    half = QUERY_KEY_ROTARY // 2
    inverse = 10000.0 ** (-jnp.arange(half, dtype=jnp.float32) * 2.0 / QUERY_KEY_ROTARY)
    angles = position[:, None] * jnp.tile(inverse, lanes // half)[None, :]
    table = jnp.stack([jnp.cos(angles), jnp.sin(angles)])
    perm, turn = spread_columns(heads)
    vmem = pl.BlockSpec(memory_space=pltpu.VMEM)
    anywhere = pl.BlockSpec(memory_space=pl.ANY)
    copies = 24 * n
    block = (share, width)
    return pl.pallas_call(
        lambda *refs: layer_kernel(n, heads, *refs),
        out_shape=jax.ShapeDtypeStruct(block, bf),
        in_specs=[vmem] + [anywhere] * 3 + [vmem] * 4 + [anywhere] * 7,
        out_specs=vmem,
        scratch_shapes=[
            pltpu.VMEM((share, rank), bf),
            pltpu.VMEM((share, rotary_key.shape[1]), bf),
            pltpu.VMEM(query_latent_rows.shape, bf),
            pltpu.VMEM(query_up_weight.shape, bf),
            pltpu.VMEM(key_value_up_weight.shape, bf),
            pltpu.VMEM(perm.shape, bf),
            pltpu.VMEM(block, bf),
            pltpu.VMEM((n, 2, 2, share, rank + lanes), bf),
            pltpu.VMEM((heads, n * rows, unit + lanes), bf),
            pltpu.VMEM((heads, rows, unit + lanes), bf),
            pltpu.VMEM((out_proj.shape[0] * 4, width), bf),
            pltpu.VMEM((heads // 2, rows, unit), bf),
            pltpu.VMEM((share, out_proj.shape[0] * 4), bf),
            pltpu.VMEM((feed_up.shape[0] * n, hid), bf),
            pltpu.VMEM((hid, feed_down.shape[1] * n), bf),
            pltpu.VMEM(block, bf),
            pltpu.VMEM((n, 2, 2, *block), bf),
            pltpu.VMEM((n, rows, hid), bf),
            pltpu.VMEM((n, 2, 2, *block), bf),
            pltpu.VMEM((n, 2, *block), bf),
            pltpu.VMEM((n, *block), bf),
            pltpu.VMEM((n, *block), bf),
            pltpu.VMEM((n, *block), bf),
            pltpu.VMEM((n, *block), bf),
            pltpu.SemaphoreType.DMA((copies,)),
            pltpu.SemaphoreType.DMA((copies,)),
            pltpu.SemaphoreType.DMA((16,)),
        ],
        compiler_params=pltpu.CompilerParams(
            collective_id=0, has_side_effects=True, vmem_limit_bytes=60 * 1024 * 1024
        ),
    )(
        table, key_value_latent, rotary_key, query_latent_rows,
        query_norm_gain.reshape(1, -1), key_value_gain.reshape(1, -1), feed_gain.reshape(1, -1), turn,
        perm, query_up_weight, key_value_up_weight, hidden_in, out_proj, feed_up, feed_down,
    )


def fits_kernel(tokens, query_up_weight, feed_up):
    n = lax.axis_size("sp")
    hid = feed_up.shape[1] // n
    heads = query_up_weight.shape[1] // (QUERY_KEY_PLAIN + QUERY_KEY_ROTARY)
    return (
        lax.axis_size("grp") == 2
        and lax.axis_size("tp") == 4
        and 1 < n
        and tokens * n <= 1024
        and tokens % 64 == 0
        and hid % 128 == 0
        and hid <= 512
        and heads * QUERY_KEY_ROTARY == 128
    )


def on_device(
    hidden_in,
    query_latent_rows,
    key_value_latent,
    rotary_key,
    query_norm_gain,
    key_value_gain,
    query_up_weight,
    key_value_up_weight,
    out_proj,
    feed_gain,
    feed_up,
    feed_down,
):
    tokens_here = hidden_in.shape[0]
    heads_here = query_up_weight.shape[1] // (QUERY_KEY_PLAIN + QUERY_KEY_ROTARY)
    position = (lax.axis_index("sp") * tokens_here + jnp.arange(tokens_here)).astype(jnp.float32)
    if fits_kernel(tokens_here, query_up_weight, feed_up):
        return run_layer(
            hidden_in, query_latent_rows, key_value_latent, rotary_key, query_norm_gain,
            key_value_gain, query_up_weight, key_value_up_weight, out_proj, feed_gain, feed_up,
            feed_down, position,
        )
    scale_factor = (QUERY_KEY_PLAIN + QUERY_KEY_ROTARY) ** (-0.5)
    query_norm = normalize(query_latent_rows, query_norm_gain).astype(jnp.bfloat16)
    queries = jnp.dot(query_norm, query_up_weight, preferred_element_type=jnp.float32).reshape(
        tokens_here, heads_here, QUERY_KEY_PLAIN + QUERY_KEY_ROTARY
    )
    queries = jnp.concatenate(
        [queries[..., :QUERY_KEY_PLAIN], rotate(queries[..., QUERY_KEY_PLAIN:], position)], axis=-1
    ).astype(jnp.bfloat16)
    query_plain = queries[..., :QUERY_KEY_PLAIN]
    query_turned = queries[..., QUERY_KEY_PLAIN:]
    latent = normalize(key_value_latent, key_value_gain).astype(jnp.bfloat16)
    key_rope = rotate(rotary_key.astype(jnp.float32), position).astype(jnp.bfloat16)

    def attend_block(carry, key_plain, value_rows, rope_rows):
        row_max, denom, accum = carry
        scores = jnp.einsum(
            "qhd,khd->hqk", query_plain, key_plain, preferred_element_type=jnp.float32
        )
        scores = scores + jnp.einsum(
            "qhd,kd->hqk", query_turned, rope_rows, preferred_element_type=jnp.float32
        )
        scores = scores * scale_factor
        new_max = jnp.maximum(row_max, jnp.max(scores, axis=-1))
        expo = jnp.exp(scores - new_max[:, :, None])
        factor = jnp.exp(row_max - new_max)
        denom = denom * factor + jnp.sum(expo, axis=-1)
        update = jnp.einsum(
            "hqk,khd->qhd",
            expo.astype(jnp.bfloat16),
            value_rows,
            preferred_element_type=jnp.float32,
        )
        accum = accum * jnp.transpose(factor)[:, :, None] + update
        return (new_max, denom, accum)

    start_carry = (
        jnp.full((heads_here, tokens_here), -1e30, jnp.float32),
        jnp.zeros((heads_here, tokens_here), jnp.float32),
        jnp.zeros((tokens_here, heads_here, VALUE_HEAD_SIZE), jnp.float32),
    )
    own_keys = jnp.dot(latent, key_value_up_weight, preferred_element_type=jnp.float32).astype(
        jnp.bfloat16
    )
    pieces = (
        lax.all_gather(own_keys, "sp", axis=0, tiled=True),
        lax.all_gather(key_rope, "sp", axis=0, tiled=True),
    )
    rows_in = pieces[0].shape[0]
    block = math.gcd(rows_in, 1024)

    def step_block(index, inner):
        first = index * block
        bulk = lax.dynamic_slice_in_dim(pieces[0], first, block, 0)
        rope_rows = lax.dynamic_slice_in_dim(pieces[1], first, block, 0)
        bulk = bulk.reshape(block, heads_here, QUERY_KEY_PLAIN + VALUE_HEAD_SIZE)
        return attend_block(
            inner, bulk[..., :QUERY_KEY_PLAIN], bulk[..., QUERY_KEY_PLAIN:], rope_rows
        )

    final_carry = lax.fori_loop(0, rows_in // block, step_block, start_carry)
    denom = final_carry[1]
    accum = final_carry[2]
    mixed = (
        (accum / jnp.transpose(denom)[:, :, None])
        .astype(jnp.bfloat16)
        .reshape(tokens_here, heads_here * VALUE_HEAD_SIZE)
    )
    up_own = lax.all_to_all(feed_up, "sp", split_axis=1, concat_axis=0, tiled=True)
    down_own = lax.all_to_all(feed_down, "sp", split_axis=0, concat_axis=1, tiled=True)
    share = tokens_here // lax.axis_size("tp")
    lead = lax.axis_index("tp") * share
    branch = lax.psum_scatter(
        jnp.dot(mixed, out_proj, preferred_element_type=jnp.float32).astype(jnp.bfloat16),
        "tp",
        scatter_dimension=0,
        tiled=True,
    ).astype(jnp.float32)
    hidden_own = lax.dynamic_slice_in_dim(hidden_in, lead, share, 0)
    middle_own = (hidden_own.astype(jnp.float32) + branch).astype(jnp.bfloat16)
    normed_own = normalize(middle_own, feed_gain).astype(jnp.bfloat16)
    normed = lax.all_gather(normed_own, ("sp", "tp"), axis=0, tiled=True)
    upward = jnp.dot(normed, up_own, preferred_element_type=jnp.float32)
    activated = jnp.square(jax.nn.relu(upward)).astype(jnp.bfloat16)
    partial_sum = jnp.dot(activated, down_own, preferred_element_type=jnp.float32)
    feed = lax.psum_scatter(
        partial_sum.astype(jnp.bfloat16), ("sp", "tp"), scatter_dimension=0, tiled=True
    ).astype(jnp.float32)
    return (middle_own.astype(jnp.float32) + feed).astype(jnp.bfloat16)


def solution(mesh):
    return jax.shard_map(
        on_device,
        mesh=mesh,
        in_specs=(
            P(("grp", "sp"), None),
            P(("grp", "sp"), None),
            P(("grp", "sp"), None),
            P(("grp", "sp"), None),
            P(),
            P(),
            P(None, "tp"),
            P(None, "tp"),
            P("tp", None),
            P(),
            P("sp", "tp"),
            P("tp", "sp"),
        ),
        out_specs=P(("grp", "sp", "tp"), None),
        check_vma=False,
    )
```

```python
import math

import jax
import jax.numpy as jnp
import numpy as np
from jax import lax
from jax.experimental import pallas as pl
from jax.experimental.pallas import tpu as pltpu
from jax.sharding import PartitionSpec as P

QUERY_KEY_PLAIN = 64
QUERY_KEY_ROTARY = 32
VALUE_HEAD_SIZE = 64


def normalize(values, gain):
    floats = values.astype(jnp.float32)
    return floats * lax.rsqrt(jnp.mean(floats * floats, axis=-1, keepdims=True) + 1e-06) * gain


def rotate(values, position):
    half_size = values.shape[-1] // 2
    inverse = 10000.0 ** (-jnp.arange(half_size, dtype=jnp.float32) * 2.0 / values.shape[-1])
    angles = position[:, None] * inverse[None, :]
    cosine = jnp.concatenate([jnp.cos(angles), jnp.cos(angles)], axis=-1)
    sine = jnp.concatenate([jnp.sin(angles), jnp.sin(angles)], axis=-1)
    shape = (values.shape[0],) + (1,) * (values.ndim - 2) + (values.shape[-1],)
    turned = jnp.concatenate([-values[..., half_size:], values[..., :half_size]], axis=-1)
    return values * cosine.reshape(shape) + turned * sine.reshape(shape)


MESH = pl.DeviceIdType.MESH


def layer_kernel(
    heads, table, kvlat, rk, qlat, gq, gkv, gain, turn, perm, wq, wkv, hidden, op, up, down, out,
    lat_in, rk_in, q_in, wq_in, wkv_in, perm_in, hid_in,
    lat_all, kv_all, q_all, op_chip, mixed, mixed_in, branch_out, branch_in, up_all, down_all, middle,
    norm_all, act, part, rf1, c2, rf2, c3, near_in, cross_out, cross_in, ss, rs, ls,
):
    n = 4
    g, me, t = lax.axis_index("grp"), lax.axis_index("sp"), lax.axis_index("tp")
    c, x = lax.rem(t, 2), t // 2
    share, width = middle.shape
    rows = share * 4
    rank = wkv.shape[0]
    piece_k = up.shape[0]
    hid = down_all.shape[0]
    half_k, half_h = piece_k // 2, hid // 2
    wide = down.shape[1]
    bf, f32 = jnp.bfloat16, jnp.float32
    vh = VALUE_HEAD_SIZE
    unit = QUERY_KEY_PLAIN + vh
    lanes = heads * QUERY_KEY_ROTARY
    scale_factor = (QUERY_KEY_PLAIN + QUERY_KEY_ROTARY) ** (-0.5)
    side = me // 2
    outer = (me == 0) | (me == n - 1)
    inner = (me == 1) | (me == n - 2)
    away = 1 - 2 * side
    partner = me + 1 - 2 * lax.rem(me, 2)
    edge, gate = side * (n - 1), 1 + side
    far_edge, far_gate = (1 - side) * (n - 1), 2 - side

    def near(i):
        if i == 0:
            return me
        if i == 1:
            return partner
        return far_gate if i == 2 else far_edge

    def at_tp(cc, xx):
        return {"tp": xx * 2 + cc}

    sib, xpeer, ypeer = at_tp(1 - c, x), at_tp(c, 1 - x), {"grp": 1 - g}
    barrier = pltpu.get_barrier_semaphore()
    for i in range(1, n):
        pl.semaphore_signal(barrier, inc=1, device_id={"sp": near(i)}, device_id_type=MESH)
    for peer in (sib, xpeer, ypeer):
        pl.semaphore_signal(barrier, inc=1, device_id=peer, device_id_type=MESH)

    def rows_of(tt):
        return pl.ds(pl.multiple_of(tt * share, share), share)

    local = []

    def fetch(src, dst):
        copy = pltpu.make_async_copy(src, dst, ls.at[len(local)])
        copy.start()
        local.append(copy)
        return copy

    got_lat = fetch(kvlat, lat_in)
    got_rk = fetch(rk, rk_in)
    got_perm = fetch(perm, perm_in)
    got_wq = fetch(wq, wq_in)
    got_q = fetch(qlat, q_in)
    got_wkv = fetch(wkv, wkv_in)
    got_op = fetch(op, op_chip.at[c])
    got_hid = fetch(hidden.at[rows_of(t)], hid_in)
    got_up = fetch(
        up.at[:, pl.ds(pl.multiple_of(me * hid, hid), hid)],
        up_all.at[pl.ds(pl.multiple_of(me * piece_k, piece_k), piece_k)],
    )
    got_down = fetch(
        down.at[pl.ds(pl.multiple_of(me * hid, hid), hid)],
        down_all.at[:, pl.ds(pl.multiple_of(me * wide, wide), wide)],
    )

    names = {}
    sent = []

    def slot(name, at):
        if name not in names:
            names[name] = sum(size for _, size in names.values()), 1 if at is None else n
        return names[name][0] + (0 if at is None else at)

    def send(name, src, dst, dev, to=None, by=None, when=None, into=None):
        copy = pltpu.make_async_remote_copy(
            src_ref=src, dst_ref=dst, send_sem=ss.at[slot(name, to)], recv_sem=rs.at[slot(into or name, by)],
            device_id=dev, device_id_type=MESH,
        )
        if when is None:
            copy.start()
        else:
            pl.when(when)(copy.start)
        sent.append((copy, when))

    def land(name, dst, by=None):
        pltpu.make_async_remote_copy(
            src_ref=dst, dst_ref=dst, send_sem=ss.at[slot(name, by)], recv_sem=rs.at[slot(name, by)],
            device_id=sib, device_id_type=MESH,
        ).wait_recv()

    def up_half(owner, hv):
        return up_all.at[pl.ds(pl.multiple_of(owner * piece_k + hv * half_k, half_k), half_k)]

    def down_half(owner, hv):
        return down_all.at[
            pl.ds(pl.multiple_of(hv * half_h, half_h), half_h),
            pl.ds(pl.multiple_of(owner * wide, wide), wide),
        ]

    def share_on(tag, buf, i):
        z = near(i)
        piece = buf.at[z, c, x]
        send((tag, "x"), piece, piece, xpeer, z, z)
        send((tag, "s"), piece, piece, sib, z, z)

    def cross(tag, buf, i):
        z = near(i)
        piece = buf.at[z, c, 1 - x]
        land((tag, "x"), piece, z)
        send((tag, "t"), piece, piece, sib, z, z)

    def settle(tag, buf, i):
        z = near(i)
        land((tag, "s"), buf.at[z, 1 - c, x], z)
        land((tag, "t"), buf.at[z, 1 - c, 1 - x], z)

    def make_latent(cc, xx):
        here = rows_of(xx * 2 + cc)
        lat_all[me, cc, xx, :, :rank] = normalize(lat_in[here, :], gkv[...]).astype(bf)
        spun = jnp.dot(rk_in[here, :], turn[...], preferred_element_type=f32)
        lat_all[me, cc, xx, :, rank:] = (
            spun[:, :lanes] * table[0, here, :] + spun[:, lanes:] * table[1, here, :]
        ).astype(bf)

    got_lat.wait()
    got_rk.wait()
    make_latent(c, x)
    pl.semaphore_wait(barrier, n + 2)
    own = lat_all.at[me, c, x]
    for i in reversed(range(1, n)):
        send(("l", "z"), own, own, {"sp": near(i)}, near(i), me)
    got_op.wait()
    send("os", op_chip.at[c], op_chip.at[c], sib)
    for cc, xx in ((1 - c, x), (c, 1 - x), (1 - c, 1 - x)):
        make_latent(cc, xx)
    got_perm.wait()
    got_wq.wait()
    wide_q = jnp.dot(wq_in[...], perm_in[...], preferred_element_type=f32).astype(bf)
    got_q.wait()
    query_norm = normalize(q_in[...], gq[...]).astype(bf)
    spread = jnp.dot(query_norm, wide_q, preferred_element_type=f32)
    first = heads * unit
    spin = (
        spread[:, first : first + lanes] * table[0] + spread[:, first + lanes : first + 2 * lanes] * table[1]
    )
    lane = lax.broadcasted_iota(jnp.int32, (rows, lanes), 1)
    for h in range(heads):
        q_all[h, :, :unit] = spread[:, h * unit : (h + 1) * unit].astype(bf)
        keep = (lane >= h * QUERY_KEY_ROTARY) & (lane < (h + 1) * QUERY_KEY_ROTARY)
        q_all[h, :, unit:] = jnp.where(keep, spin, 0.0).astype(bf)

    for i in range(1, n):
        land(("l", "z"), lat_all.at[near(i), c, x], near(i))
        share_on("l", lat_all, i)
    for i in reversed(range(1, n)):
        send(
            "up",
            up.at[
                pl.ds(pl.multiple_of(g * half_k, half_k), half_k),
                pl.ds(pl.multiple_of(near(i) * hid, hid), hid),
            ],
            up_half(me, g),
            {"sp": near(i)},
            near(i),
            me,
        )
    got_wkv.wait()
    for i in range(1, n):
        cross("l", lat_all, i)
    for i in range(1, n):
        settle("l", lat_all, i)
    for j in range(n):
        made = jnp.dot(
            lat_all[j, :, :, :, :rank].reshape(rows, rank), wkv_in[...], preferred_element_type=f32
        ).astype(bf)
        rope = lat_all[j, :, :, :, rank:].reshape(rows, lanes)
        for h in range(heads):
            kv_all[h, j * rows : (j + 1) * rows, :unit] = made[:, h * unit : (h + 1) * unit]
            kv_all[h, j * rows : (j + 1) * rows, unit:] = rope

    contract = (((1,), (1,)), ((), ()))
    low = lax.broadcasted_iota(jnp.int32, (rows, unit), 1) < vh

    def attend(h):
        scores = lax.dot_general(q_all[h], kv_all[h], contract, preferred_element_type=f32)
        scores = scores * scale_factor
        expo = jnp.exp(scores - jnp.max(scores, axis=-1, keepdims=True))
        total = jnp.sum(expo, axis=-1, keepdims=True)
        mix = jnp.dot(expo.astype(bf), kv_all[h, :, :unit], preferred_element_type=f32)
        return mix / total

    def head_cols(cc, p):
        return pl.ds(pl.multiple_of(cc * heads * vh + p * unit, unit), unit)

    for p in range(heads // 2):
        left, right = attend(2 * p), attend(2 * p + 1)
        pair = jnp.where(low, pltpu.roll(left, vh, 1), right)
        mixed[p] = pair.astype(bf)
        for xx in range(2):
            send(
                ("m", p, xx), mixed.at[p, rows_of(xx * 2 + 1 - c)], mixed_in.at[xx, :, head_cols(c, p)], sib
            )
            mixed_in[xx, :, head_cols(c, p)] = mixed[p, rows_of(xx * 2 + c), :]

    land("os", op_chip.at[1 - c])
    for p in range(heads // 2):
        for xx in range(2):
            land(("m", p, xx), mixed_in.at[xx, :, head_cols(1 - c, p)])

    tiles = width // wide
    chip_heads = 2 * heads * vh

    def project(xx, j):
        return jnp.dot(
            mixed_in[xx],
            op_chip[:, :, j * wide : (j + 1) * wide].reshape(chip_heads, wide),
            preferred_element_type=f32,
        )

    for j in range(tiles):
        branch_out[j] = project(1 - x, j).astype(bf)
        send(("b", j), branch_out.at[j], branch_in.at[j], xpeer)
    got_hid.wait()
    for j in range(tiles):
        kept = project(x, j)
        land(("b", j), branch_in.at[j])
        cols = slice(j * wide, (j + 1) * wide)
        middle[:, cols] = (hid_in[:, cols].astype(f32) + (kept + branch_in[j].astype(f32))).astype(bf)
    norm_all[me, c, x] = normalize(middle[...], gain[...]).astype(bf)

    def pass_on(i, to, when):
        z = near(i)
        send(("n", "z"), norm_all.at[z, c, x], norm_all.at[z, c, x], {"sp": to}, z, z, when)

    def send_down(i, when):
        send(
            "dn",
            down.at[pl.ds(pl.multiple_of(near(i) * hid + g * half_h, half_h), half_h)],
            down_half(me, g),
            {"sp": near(i)},
            near(i),
            me,
            when,
        )

    own = norm_all.at[me, c, x]
    send(("n", "z"), own, own, {"sp": partner}, me, me)
    send(("n", "c"), own, own, {"sp": far_gate}, None, me, inner, ("n", "z"))
    share_on("n", norm_all, 0)
    for i in range(1, n):
        piece = up_half(near(i), g)
        land("up", piece, near(i))
        send("uy", piece, piece, ypeer, near(i), near(i))

    def raise_block(i):
        z = near(i)
        upward = jnp.dot(norm_all[z].reshape(rows, width), up_all[...], preferred_element_type=f32)
        act[z] = jnp.square(jnp.maximum(upward, 0.0)).astype(bf)

    def relay(i, to):
        land(("n", "z"), norm_all.at[near(i), c, x], near(i))
        pass_on(i, to, inner)
        share_on("n", norm_all, i)

    relay(1, far_gate)
    send_down(3, inner)
    send_down(2, inner)
    cross("n", norm_all, 0)
    relay(2, partner)
    for i in reversed(range(1, n)):
        send_down(i, outer)
    for i in range(1, n):
        land("uy", up_half(near(i), 1 - g), near(i))
    got_up.wait()
    settle("n", norm_all, 0)
    raise_block(0)
    cross("n", norm_all, 1)
    relay(3, partner)
    send_down(1, inner)
    settle("n", norm_all, 1)
    raise_block(1)
    cross("n", norm_all, 2)
    settle("n", norm_all, 2)
    raise_block(2)
    cross("n", norm_all, 3)
    settle("n", norm_all, 3)
    raise_block(3)

    def forward(j):
        piece = down_half(j, g)

        @pl.when(me != j)
        def _():
            land("dn", piece, j)

        send("dy", piece, piece, ypeer, j, j, me != j)

    def arrive(j):
        @pl.when(me != j)
        def _():
            land("dy", down_half(j, 1 - g), j)

    def lower(j):
        @pl.loop(0, n)
        def _(d):
            made = jnp.dot(act[d], down_all[:, j * wide : (j + 1) * wide], preferred_element_type=f32)
            made = made.astype(bf).reshape(2, 2, share, wide)
            part[j, 0, d] = made[0]
            part[j, 1, d] = made[1]

        send(("f1", j), part.at[j, 1 - c], rf1.at[j], sib)

    def fold_core(j):
        land(("f1", j), rf1.at[j])
        c2[j] = (part[j, c, :, 1 - x].astype(f32) + rf1[j, :, 1 - x].astype(f32)).astype(bf)
        send(("f2", j), c2.at[j], rf2.at[j], xpeer)

    def fold_x(j):
        land(("f2", j), rf2.at[j])
        c3[j] = (
            part[j, c, :, x].astype(f32) + rf1[j, :, x].astype(f32) + rf2[j].astype(f32)
        ).astype(bf)
        send(("pe", j), c3.at[j, far_edge], near_in.at[j, 2], {"sp": partner}, None, None, outer)
        send(("pg", j), c3.at[j, far_gate], near_in.at[j, 1], {"sp": partner}, None, None, outer)
        send(("p", j), c3.at[j, partner], near_in.at[j, 0], {"sp": partner})

    def fold_side(j):
        @pl.when(inner)
        def _():
            land(("pe", j), near_in.at[j, 2])
            cross_out[j, 1] = (c3[j, far_edge].astype(f32) + near_in[j, 2].astype(f32)).astype(bf)

        send(("q", j, 1), cross_out.at[j, 1], cross_in.at[j], {"sp": far_edge}, None, None, inner, ("q", j))

        @pl.when(inner)
        def _():
            land(("pg", j), near_in.at[j, 1])
            cross_out[j, 0] = (c3[j, far_gate].astype(f32) + near_in[j, 1].astype(f32)).astype(bf)

        send(("q", j, 0), cross_out.at[j, 0], cross_in.at[j], {"sp": far_gate}, None, None, inner, ("q", j))

    def finish(j):
        cols = slice(j * wide, (j + 1) * wide)
        land(("p", j), near_in.at[j, 0])
        land(("q", j), cross_in.at[j])
        feed = c3[j, me].astype(f32) + near_in[j, 0].astype(f32) + cross_in[j].astype(f32)
        out[:, cols] = (middle[:, cols].astype(f32) + feed).astype(bf)

    order = (1, 2, 0, 3)
    forward(order[0])
    got_down.wait()
    for at, j in enumerate(order):
        arrive(j)
        lower(j)
        if at:
            fold_x(order[at - 1])
        fold_core(j)
        if at > 1:
            fold_side(order[at - 2])
        if at + 1 < n:
            forward(order[at + 1])
    fold_x(order[3])
    fold_side(order[2])
    fold_side(order[3])
    for j in order:
        finish(j)
    for copy, when in sent:
        if when is None:
            copy.wait_send()
        else:
            pl.when(when)(copy.wait_send)


def spread_columns(heads):
    head = QUERY_KEY_PLAIN + QUERY_KEY_ROTARY
    half = QUERY_KEY_ROTARY // 2
    unit = QUERY_KEY_PLAIN + VALUE_HEAD_SIZE
    lanes = heads * QUERY_KEY_ROTARY
    perm = np.zeros((heads * head, heads * unit + 2 * lanes), np.float32)
    turn = np.zeros((QUERY_KEY_ROTARY, 2 * lanes), np.float32)
    for h in range(heads):
        for r in range(QUERY_KEY_PLAIN):
            perm[h * head + r, h * unit + r] = 1.0
        for r in range(QUERY_KEY_ROTARY):
            col = h * QUERY_KEY_ROTARY + r
            other, sign = (r + half, -1.0) if r < half else (r - half, 1.0)
            turn[r, col] = 1.0
            turn[other, lanes + col] = sign
            perm[h * head + QUERY_KEY_PLAIN + r, heads * unit + col] = 1.0
            perm[h * head + QUERY_KEY_PLAIN + other, heads * unit + lanes + col] = sign
    return jnp.asarray(perm, jnp.bfloat16), jnp.asarray(turn, jnp.bfloat16)


def run_layer(
    hidden_in, query_latent_rows, key_value_latent, rotary_key, query_norm_gain, key_value_gain,
    query_up_weight, key_value_up_weight, out_proj, feed_gain, feed_up, feed_down, position,
):
    n = lax.axis_size("sp")
    rows, width = hidden_in.shape
    heads = query_up_weight.shape[1] // (QUERY_KEY_PLAIN + QUERY_KEY_ROTARY)
    share = rows // lax.axis_size("tp")
    hid = feed_up.shape[1] // n
    unit = QUERY_KEY_PLAIN + VALUE_HEAD_SIZE
    lanes = heads * QUERY_KEY_ROTARY
    rank = key_value_latent.shape[1]
    bf = jnp.bfloat16
    half = QUERY_KEY_ROTARY // 2
    inverse = 10000.0 ** (-jnp.arange(half, dtype=jnp.float32) * 2.0 / QUERY_KEY_ROTARY)
    angles = position[:, None] * jnp.tile(inverse, lanes // half)[None, :]
    table = jnp.stack([jnp.cos(angles), jnp.sin(angles)])
    perm, turn = spread_columns(heads)
    vmem = pl.BlockSpec(memory_space=pltpu.VMEM)
    anywhere = pl.BlockSpec(memory_space=pl.ANY)
    wide = width // n
    copies = 32 * n
    block = (share, width)
    return pl.pallas_call(
        lambda *refs: layer_kernel(heads, *refs),
        out_shape=jax.ShapeDtypeStruct(block, bf),
        in_specs=[vmem] + [anywhere] * 3 + [vmem] * 4 + [anywhere] * 7,
        out_specs=vmem,
        scratch_shapes=[
            pltpu.VMEM(key_value_latent.shape, bf),
            pltpu.VMEM(rotary_key.shape, bf),
            pltpu.VMEM(query_latent_rows.shape, bf),
            pltpu.VMEM(query_up_weight.shape, bf),
            pltpu.VMEM(key_value_up_weight.shape, bf),
            pltpu.VMEM(perm.shape, bf),
            pltpu.VMEM(block, bf),
            pltpu.VMEM((n, 2, 2, share, rank + lanes), bf),
            pltpu.VMEM((heads, n * rows, unit + lanes), bf),
            pltpu.VMEM((heads, rows, unit + lanes), bf),
            pltpu.VMEM((2, *out_proj.shape), bf),
            pltpu.VMEM((heads // 2, rows, unit), bf),
            pltpu.VMEM((2, share, out_proj.shape[0] * 2), bf),
            pltpu.VMEM((n, share, wide), bf),
            pltpu.VMEM((n, share, wide), bf),
            pltpu.VMEM((feed_up.shape[0] * n, hid), bf),
            pltpu.VMEM((hid, width), bf),
            pltpu.VMEM(block, bf),
            pltpu.VMEM((n, 2, 2, *block), bf),
            pltpu.VMEM((n, rows, hid), bf),
            pltpu.VMEM((n, 2, n, 2, share, wide), bf),
            pltpu.VMEM((n, n, 2, share, wide), bf),
            pltpu.VMEM((n, n, share, wide), bf),
            pltpu.VMEM((n, n, share, wide), bf),
            pltpu.VMEM((n, n, share, wide), bf),
            pltpu.VMEM((n, 3, share, wide), bf),
            pltpu.VMEM((n, 2, share, wide), bf),
            pltpu.VMEM((n, share, wide), bf),
            pltpu.SemaphoreType.DMA((copies,)),
            pltpu.SemaphoreType.DMA((copies,)),
            pltpu.SemaphoreType.DMA((16,)),
        ],
        compiler_params=pltpu.CompilerParams(
            collective_id=0, has_side_effects=True, vmem_limit_bytes=60 * 1024 * 1024
        ),
    )(
        table, key_value_latent, rotary_key, query_latent_rows,
        query_norm_gain.reshape(1, -1), key_value_gain.reshape(1, -1), feed_gain.reshape(1, -1), turn,
        perm, query_up_weight, key_value_up_weight, hidden_in, out_proj, feed_up, feed_down,
    )


def fits_kernel(tokens, query_up_weight, feed_up):
    n = lax.axis_size("sp")
    hid = feed_up.shape[1] // n
    heads = query_up_weight.shape[1] // (QUERY_KEY_PLAIN + QUERY_KEY_ROTARY)
    return (
        lax.axis_size("grp") == 2
        and lax.axis_size("tp") == 4
        and n == 4
        and tokens * n <= 1024
        and tokens % 64 == 0
        and hid % 128 == 0
        and hid <= 512
        and heads * QUERY_KEY_ROTARY == 128
    )


def on_device(
    hidden_in,
    query_latent_rows,
    key_value_latent,
    rotary_key,
    query_norm_gain,
    key_value_gain,
    query_up_weight,
    key_value_up_weight,
    out_proj,
    feed_gain,
    feed_up,
    feed_down,
):
    tokens_here = hidden_in.shape[0]
    heads_here = query_up_weight.shape[1] // (QUERY_KEY_PLAIN + QUERY_KEY_ROTARY)
    position = (lax.axis_index("sp") * tokens_here + jnp.arange(tokens_here)).astype(jnp.float32)
    if fits_kernel(tokens_here, query_up_weight, feed_up):
        return run_layer(
            hidden_in, query_latent_rows, key_value_latent, rotary_key, query_norm_gain,
            key_value_gain, query_up_weight, key_value_up_weight, out_proj, feed_gain, feed_up,
            feed_down, position,
        )
    scale_factor = (QUERY_KEY_PLAIN + QUERY_KEY_ROTARY) ** (-0.5)
    query_norm = normalize(query_latent_rows, query_norm_gain).astype(jnp.bfloat16)
    queries = jnp.dot(query_norm, query_up_weight, preferred_element_type=jnp.float32).reshape(
        tokens_here, heads_here, QUERY_KEY_PLAIN + QUERY_KEY_ROTARY
    )
    queries = jnp.concatenate(
        [queries[..., :QUERY_KEY_PLAIN], rotate(queries[..., QUERY_KEY_PLAIN:], position)], axis=-1
    ).astype(jnp.bfloat16)
    query_plain = queries[..., :QUERY_KEY_PLAIN]
    query_turned = queries[..., QUERY_KEY_PLAIN:]
    latent = normalize(key_value_latent, key_value_gain).astype(jnp.bfloat16)
    key_rope = rotate(rotary_key.astype(jnp.float32), position).astype(jnp.bfloat16)

    def attend_block(carry, key_plain, value_rows, rope_rows):
        row_max, denom, accum = carry
        scores = jnp.einsum(
            "qhd,khd->hqk", query_plain, key_plain, preferred_element_type=jnp.float32
        )
        scores = scores + jnp.einsum(
            "qhd,kd->hqk", query_turned, rope_rows, preferred_element_type=jnp.float32
        )
        scores = scores * scale_factor
        new_max = jnp.maximum(row_max, jnp.max(scores, axis=-1))
        expo = jnp.exp(scores - new_max[:, :, None])
        factor = jnp.exp(row_max - new_max)
        denom = denom * factor + jnp.sum(expo, axis=-1)
        update = jnp.einsum(
            "hqk,khd->qhd",
            expo.astype(jnp.bfloat16),
            value_rows,
            preferred_element_type=jnp.float32,
        )
        accum = accum * jnp.transpose(factor)[:, :, None] + update
        return (new_max, denom, accum)

    start_carry = (
        jnp.full((heads_here, tokens_here), -1e30, jnp.float32),
        jnp.zeros((heads_here, tokens_here), jnp.float32),
        jnp.zeros((tokens_here, heads_here, VALUE_HEAD_SIZE), jnp.float32),
    )
    own_keys = jnp.dot(latent, key_value_up_weight, preferred_element_type=jnp.float32).astype(
        jnp.bfloat16
    )
    pieces = (
        lax.all_gather(own_keys, "sp", axis=0, tiled=True),
        lax.all_gather(key_rope, "sp", axis=0, tiled=True),
    )
    rows_in = pieces[0].shape[0]
    block = math.gcd(rows_in, 1024)

    def step_block(index, inner):
        first = index * block
        bulk = lax.dynamic_slice_in_dim(pieces[0], first, block, 0)
        rope_rows = lax.dynamic_slice_in_dim(pieces[1], first, block, 0)
        bulk = bulk.reshape(block, heads_here, QUERY_KEY_PLAIN + VALUE_HEAD_SIZE)
        return attend_block(
            inner, bulk[..., :QUERY_KEY_PLAIN], bulk[..., QUERY_KEY_PLAIN:], rope_rows
        )

    final_carry = lax.fori_loop(0, rows_in // block, step_block, start_carry)
    denom = final_carry[1]
    accum = final_carry[2]
    mixed = (
        (accum / jnp.transpose(denom)[:, :, None])
        .astype(jnp.bfloat16)
        .reshape(tokens_here, heads_here * VALUE_HEAD_SIZE)
    )
    up_own = lax.all_to_all(feed_up, "sp", split_axis=1, concat_axis=0, tiled=True)
    down_own = lax.all_to_all(feed_down, "sp", split_axis=0, concat_axis=1, tiled=True)
    share = tokens_here // lax.axis_size("tp")
    lead = lax.axis_index("tp") * share
    branch = lax.psum_scatter(
        jnp.dot(mixed, out_proj, preferred_element_type=jnp.float32).astype(jnp.bfloat16),
        "tp",
        scatter_dimension=0,
        tiled=True,
    ).astype(jnp.float32)
    hidden_own = lax.dynamic_slice_in_dim(hidden_in, lead, share, 0)
    middle_own = (hidden_own.astype(jnp.float32) + branch).astype(jnp.bfloat16)
    normed_own = normalize(middle_own, feed_gain).astype(jnp.bfloat16)
    normed = lax.all_gather(normed_own, ("sp", "tp"), axis=0, tiled=True)
    upward = jnp.dot(normed, up_own, preferred_element_type=jnp.float32)
    activated = jnp.square(jax.nn.relu(upward)).astype(jnp.bfloat16)
    partial_sum = jnp.dot(activated, down_own, preferred_element_type=jnp.float32)
    feed = lax.psum_scatter(
        partial_sum.astype(jnp.bfloat16), ("sp", "tp"), scatter_dimension=0, tiled=True
    ).astype(jnp.float32)
    return (middle_own.astype(jnp.float32) + feed).astype(jnp.bfloat16)


def solution(mesh):
    return jax.shard_map(
        on_device,
        mesh=mesh,
        in_specs=(
            P(("grp", "sp"), None),
            P(("grp", "sp"), None),
            P(("grp", "sp"), None),
            P(("grp", "sp"), None),
            P(),
            P(),
            P(None, "tp"),
            P(None, "tp"),
            P("tp", None),
            P(),
            P("sp", "tp"),
            P("tp", "sp"),
        ),
        out_specs=P(("grp", "sp", "tp"), None),
        check_vma=False,
    )
```

```python
import math

import jax
import jax.numpy as jnp
import numpy as np
from jax import lax
from jax.experimental import pallas as pl
from jax.experimental.pallas import tpu as pltpu
from jax.sharding import PartitionSpec as P

QUERY_KEY_PLAIN = 64
QUERY_KEY_ROTARY = 32
VALUE_HEAD_SIZE = 64


def normalize(values, gain):
    floats = values.astype(jnp.float32)
    return floats * lax.rsqrt(jnp.mean(floats * floats, axis=-1, keepdims=True) + 1e-06) * gain


def rotate(values, position):
    half_size = values.shape[-1] // 2
    inverse = 10000.0 ** (-jnp.arange(half_size, dtype=jnp.float32) * 2.0 / values.shape[-1])
    angles = position[:, None] * inverse[None, :]
    cosine = jnp.concatenate([jnp.cos(angles), jnp.cos(angles)], axis=-1)
    sine = jnp.concatenate([jnp.sin(angles), jnp.sin(angles)], axis=-1)
    shape = (values.shape[0],) + (1,) * (values.ndim - 2) + (values.shape[-1],)
    turned = jnp.concatenate([-values[..., half_size:], values[..., :half_size]], axis=-1)
    return values * cosine.reshape(shape) + turned * sine.reshape(shape)


MESH = pl.DeviceIdType.MESH


def layer_kernel(
    heads, table, kvlat, rk, qlat, gq, gkv, gain, turn, perm, wq, wkv, hidden, op, up, down, out,
    lat_in, rk_in, q_in, wq_in, wkv_in, perm_in, hid_in,
    lat_all, kv_all, q_all, op_chip, mixed, mixed_in, branch_out, branch_in, up_all, down_all, middle,
    norm_all, act, part, rf1, c2, rf2, c3, near_in, cross_out, cross_in, ss, rs, ls,
):
    n = 4
    g, me, t = lax.axis_index("grp"), lax.axis_index("sp"), lax.axis_index("tp")
    c, x = lax.rem(t, 2), t // 2
    share, width = middle.shape
    rows = share * 4
    rank = wkv.shape[0]
    piece_k = up.shape[0]
    hid = down_all.shape[0]
    half_k, half_h = piece_k // 2, hid // 2
    wide = down.shape[1]
    bf, f32 = jnp.bfloat16, jnp.float32
    vh = VALUE_HEAD_SIZE
    unit = QUERY_KEY_PLAIN + vh
    lanes = heads * QUERY_KEY_ROTARY
    scale_factor = (QUERY_KEY_PLAIN + QUERY_KEY_ROTARY) ** (-0.5)
    side = me // 2
    outer = (me == 0) | (me == n - 1)
    inner = (me == 1) | (me == n - 2)
    away = 1 - 2 * side
    partner = me + 1 - 2 * lax.rem(me, 2)
    edge, gate = side * (n - 1), 1 + side
    far_edge, far_gate = (1 - side) * (n - 1), 2 - side

    def near(i):
        if i == 0:
            return me
        if i == 1:
            return partner
        return far_gate if i == 2 else far_edge

    def at_tp(cc, xx):
        return {"tp": xx * 2 + cc}

    sib, xpeer, ypeer = at_tp(1 - c, x), at_tp(c, 1 - x), {"grp": 1 - g}
    barrier = pltpu.get_barrier_semaphore()
    for i in range(1, n):
        pl.semaphore_signal(barrier, inc=1, device_id={"sp": near(i)}, device_id_type=MESH)
    for peer in (sib, xpeer, ypeer):
        pl.semaphore_signal(barrier, inc=1, device_id=peer, device_id_type=MESH)

    def rows_of(tt):
        return pl.ds(pl.multiple_of(tt * share, share), share)

    local = []

    def fetch(src, dst):
        copy = pltpu.make_async_copy(src, dst, ls.at[len(local)])
        copy.start()
        local.append(copy)
        return copy

    got_lat = fetch(kvlat, lat_in)
    got_rk = fetch(rk, rk_in)
    got_perm = fetch(perm, perm_in)
    got_wq = fetch(wq, wq_in)
    got_q = fetch(qlat, q_in)
    got_wkv = fetch(wkv, wkv_in)
    got_op = fetch(op, op_chip.at[c])
    got_hid = fetch(hidden.at[rows_of(t)], hid_in)
    got_up = fetch(
        up.at[:, pl.ds(pl.multiple_of(me * hid, hid), hid)],
        up_all.at[pl.ds(pl.multiple_of(me * piece_k, piece_k), piece_k)],
    )
    got_down = fetch(
        down.at[pl.ds(pl.multiple_of(me * hid, hid), hid)],
        down_all.at[:, pl.ds(pl.multiple_of(me * wide, wide), wide)],
    )

    names = {}
    sent = []

    def slot(name, at):
        if name not in names:
            names[name] = sum(size for _, size in names.values()), 1 if at is None else n
        return names[name][0] + (0 if at is None else at)

    def send(name, src, dst, dev, to=None, by=None, when=None, into=None):
        copy = pltpu.make_async_remote_copy(
            src_ref=src, dst_ref=dst, send_sem=ss.at[slot(name, to)], recv_sem=rs.at[slot(into or name, by)],
            device_id=dev, device_id_type=MESH,
        )
        if when is None:
            copy.start()
        else:
            pl.when(when)(copy.start)
        sent.append((copy, when))

    def land(name, dst, by=None):
        pltpu.make_async_remote_copy(
            src_ref=dst, dst_ref=dst, send_sem=ss.at[slot(name, by)], recv_sem=rs.at[slot(name, by)],
            device_id=sib, device_id_type=MESH,
        ).wait_recv()

    def up_half(owner, hv):
        return up_all.at[pl.ds(pl.multiple_of(owner * piece_k + hv * half_k, half_k), half_k)]

    def down_half(owner, hv):
        return down_all.at[
            pl.ds(pl.multiple_of(hv * half_h, half_h), half_h),
            pl.ds(pl.multiple_of(owner * wide, wide), wide),
        ]

    def share_on(tag, buf, i):
        z = near(i)
        piece = buf.at[z, c, x]
        send((tag, "x"), piece, piece, xpeer, z, z)
        send((tag, "s"), piece, piece, sib, z, z)

    def cross(tag, buf, i):
        z = near(i)
        piece = buf.at[z, c, 1 - x]
        land((tag, "x"), piece, z)
        send((tag, "t"), piece, piece, sib, z, z)

    def settle(tag, buf, i, both=True):
        z = near(i)
        if both:
            land((tag, "s"), buf.at[z, 1 - c, x], z)
        land((tag, "t"), buf.at[z, 1 - c, 1 - x], z)

    def make_latent(cc, xx):
        here = rows_of(xx * 2 + cc)
        lat_all[me, cc, xx, :, :rank] = normalize(lat_in[here, :], gkv[...]).astype(bf)
        spun = jnp.dot(rk_in[here, :], turn[...], preferred_element_type=f32)
        lat_all[me, cc, xx, :, rank:] = (
            spun[:, :lanes] * table[0, here, :] + spun[:, lanes:] * table[1, here, :]
        ).astype(bf)

    got_lat.wait()
    got_rk.wait()
    make_latent(c, x)
    pl.semaphore_wait(barrier, n + 2)
    own = lat_all.at[me, c, x]
    for i in reversed(range(1, n)):
        send(("l", "z"), own, own, {"sp": near(i)}, near(i), me)
    got_op.wait()
    send("os", op_chip.at[c], op_chip.at[c], sib)
    for cc, xx in ((1 - c, x), (c, 1 - x), (1 - c, 1 - x)):
        make_latent(cc, xx)
    got_perm.wait()
    got_wq.wait()
    wide_q = jnp.dot(wq_in[...], perm_in[...], preferred_element_type=f32).astype(bf)
    got_q.wait()
    query_norm = normalize(q_in[...], gq[...]).astype(bf)
    spread = jnp.dot(query_norm, wide_q, preferred_element_type=f32)
    first = heads * unit
    spin = (
        spread[:, first : first + lanes] * table[0] + spread[:, first + lanes : first + 2 * lanes] * table[1]
    )
    lane = lax.broadcasted_iota(jnp.int32, (rows, lanes), 1)
    for h in range(heads):
        q_all[h, :, :unit] = spread[:, h * unit : (h + 1) * unit].astype(bf)
        keep = (lane >= h * QUERY_KEY_ROTARY) & (lane < (h + 1) * QUERY_KEY_ROTARY)
        q_all[h, :, unit:] = jnp.where(keep, spin, 0.0).astype(bf)

    land(("l", "z"), lat_all.at[near(1), c, x], near(1))
    share_on("l", lat_all, 1)
    land(("l", "z"), lat_all.at[near(2), c, x], near(2))
    share_on("l", lat_all, 2)
    land(("l", "z"), lat_all.at[near(3), c, x], near(3))
    share_on("l", lat_all, 3)
    def send_up(i, when):
        send(
            "up",
            up.at[
                pl.ds(pl.multiple_of(g * half_k, half_k), half_k),
                pl.ds(pl.multiple_of(near(i) * hid, hid), hid),
            ],
            up_half(me, g),
            {"sp": near(i)},
            near(i),
            me,
            when,
        )

    send_up(3, inner)
    send_up(1, None)
    got_wkv.wait()
    for i in range(1, n):
        cross("l", lat_all, i)
    send_up(3, outer)
    send_up(2, outer)
    for i in range(1, n):
        settle("l", lat_all, i)
    for j in range(n):
        made = jnp.dot(
            lat_all[j, :, :, :, :rank].reshape(rows, rank), wkv_in[...], preferred_element_type=f32
        ).astype(bf)
        rope = lat_all[j, :, :, :, rank:].reshape(rows, lanes)
        for h in range(heads):
            kv_all[h, j * rows : (j + 1) * rows, :unit] = made[:, h * unit : (h + 1) * unit]
            kv_all[h, j * rows : (j + 1) * rows, unit:] = rope

    contract = (((1,), (1,)), ((), ()))
    low = lax.broadcasted_iota(jnp.int32, (rows, unit), 1) < vh

    def attend(h):
        scores = lax.dot_general(q_all[h], kv_all[h], contract, preferred_element_type=f32)
        scores = scores * scale_factor
        expo = jnp.exp(scores - jnp.max(scores, axis=-1, keepdims=True))
        total = jnp.sum(expo, axis=-1, keepdims=True)
        mix = jnp.dot(expo.astype(bf), kv_all[h, :, :unit], preferred_element_type=f32)
        return mix / total

    def head_cols(cc, p):
        return pl.ds(pl.multiple_of(cc * heads * vh + p * unit, unit), unit)

    for p in range(heads // 2):
        left, right = attend(2 * p), attend(2 * p + 1)
        pair = jnp.where(low, pltpu.roll(left, vh, 1), right)
        mixed[p] = pair.astype(bf)
        for xx in range(2):
            send(
                ("m", p, xx), mixed.at[p, rows_of(xx * 2 + 1 - c)], mixed_in.at[xx, :, head_cols(c, p)], sib
            )
            mixed_in[xx, :, head_cols(c, p)] = mixed[p, rows_of(xx * 2 + c), :]

    land("os", op_chip.at[1 - c])
    for p in range(heads // 2):
        for xx in range(2):
            land(("m", p, xx), mixed_in.at[xx, :, head_cols(1 - c, p)])

    tiles = width // wide
    chip_heads = 2 * heads * vh

    def project(xx, j):
        return jnp.dot(
            mixed_in[xx],
            op_chip[:, :, j * wide : (j + 1) * wide].reshape(chip_heads, wide),
            preferred_element_type=f32,
        )

    for j in range(tiles):
        branch_out[j] = project(1 - x, j).astype(bf)
        send(("b", j), branch_out.at[j], branch_in.at[j], xpeer)
    got_hid.wait()
    for j in range(tiles):
        kept = project(x, j)
        land(("b", j), branch_in.at[j])
        cols = slice(j * wide, (j + 1) * wide)
        middle[:, cols] = (hid_in[:, cols].astype(f32) + (kept + branch_in[j].astype(f32))).astype(bf)
    norm_all[me, c, x] = normalize(middle[...], gain[...]).astype(bf)

    def pass_on(i, to, when):
        z = near(i)
        send(("n", "z"), norm_all.at[z, c, x], norm_all.at[z, c, x], {"sp": to}, z, z, when)

    def send_down(i, when):
        send(
            "dn",
            down.at[pl.ds(pl.multiple_of(near(i) * hid + g * half_h, half_h), half_h)],
            down_half(me, g),
            {"sp": near(i)},
            near(i),
            me,
            when,
        )

    own = norm_all.at[me, c, x]
    send(("n", "z"), own, own, {"sp": partner}, me, me)
    send(("n", "c"), own, own, {"sp": far_gate}, None, me, inner, ("n", "z"))
    share_on("n", norm_all, 0)
    send_down(1, outer)
    def forward_up(i, when):
        piece = up_half(near(i), g)
        if when is None:
            land("up", piece, near(i))
        else:
            pl.when(when)(lambda: land("up", piece, near(i)))
        send("uy", piece, piece, ypeer, near(i), near(i), when)

    forward_up(1, None)
    forward_up(2, outer)
    forward_up(3, None)

    def raise_block(i):
        z = near(i)
        upward = jnp.dot(norm_all[z].reshape(rows, width), up_all[...], preferred_element_type=f32)
        act[z] = jnp.square(jnp.maximum(upward, 0.0)).astype(bf)

    def relay(i, to):
        land(("n", "z"), norm_all.at[near(i), c, x], near(i))
        pass_on(i, to, inner)
        share_on("n", norm_all, i)

    def forward(i, when):
        j = near(i)
        piece = down_half(j, g)
        if when is None:
            land("dn", piece, j)
        else:
            pl.when(when)(lambda: land("dn", piece, j))
        send("dy", piece, piece, ypeer, j, j, when)

    relay(1, far_gate)
    send_up(2, inner)
    cross("n", norm_all, 0)
    relay(2, partner)
    cross("n", norm_all, 1)
    relay(3, partner)
    land(("n", "s"), norm_all.at[near(3), 1 - c, x], near(3))
    send_down(2, inner)
    send_down(3, outer)
    send_down(2, outer)
    forward_up(2, inner)
    cross("n", norm_all, 2)
    send_down(3, inner)
    send_down(1, inner)
    for i in range(1, n):
        land("uy", up_half(near(i), 1 - g), near(i))
    got_up.wait()
    settle("n", norm_all, 0)
    raise_block(0)
    cross("n", norm_all, 3)
    settle("n", norm_all, 1)
    raise_block(1)
    settle("n", norm_all, 2)
    raise_block(2)
    forward(1, inner)
    settle("n", norm_all, 3, False)
    raise_block(3)

    def block(j):
        return pl.ds(pl.multiple_of(j * wide, wide), wide)

    def arrive(i):
        if i:
            land("dy", down_half(near(i), 1 - g), near(i))
        else:
            got_down.wait()

    def lower(i):
        j = near(i)

        @pl.loop(0, n)
        def _(d):
            made = jnp.dot(act[d], down_all[:, block(j)], preferred_element_type=f32)
            made = made.astype(bf).reshape(2, 2, share, wide)
            part[j, 0, d] = made[0]
            part[j, 1, d] = made[1]

        send("f1", part.at[j, 1 - c], rf1.at[j], sib, j, j)

    def fold_core(i):
        j = near(i)
        land("f1", rf1.at[j], j)
        c2[j] = (part[j, c, :, 1 - x].astype(f32) + rf1[j, :, 1 - x].astype(f32)).astype(bf)
        send("f2", c2.at[j], rf2.at[j], xpeer, j, j)

    def fold_x(i):
        j = near(i)
        land("f2", rf2.at[j], j)
        c3[j] = (
            part[j, c, :, x].astype(f32) + rf1[j, :, x].astype(f32) + rf2[j].astype(f32)
        ).astype(bf)
        send("pe", c3.at[j, far_edge], near_in.at[j, 2], {"sp": partner}, j, j, outer)
        send("pg", c3.at[j, far_gate], near_in.at[j, 1], {"sp": partner}, j, j, outer)
        send("p", c3.at[j, partner], near_in.at[j, 0], {"sp": partner}, j, j)

    def fold_side(i):
        j = near(i)

        @pl.when(inner)
        def _():
            land("pe", near_in.at[j, 2], j)
            cross_out[j, 1] = (c3[j, far_edge].astype(f32) + near_in[j, 2].astype(f32)).astype(bf)

        send("q1", cross_out.at[j, 1], cross_in.at[j], {"sp": far_edge}, j, j, inner, "q0")

        @pl.when(inner)
        def _():
            land("pg", near_in.at[j, 1], j)
            cross_out[j, 0] = (c3[j, far_gate].astype(f32) + near_in[j, 1].astype(f32)).astype(bf)

        send("q0", cross_out.at[j, 0], cross_in.at[j], {"sp": far_gate}, j, j, inner)

    def finish(i):
        j = near(i)
        land("p", near_in.at[j, 0], j)
        land("q0", cross_in.at[j], j)
        feed = c3[j, me].astype(f32) + near_in[j, 0].astype(f32) + cross_in[j].astype(f32)
        out[:, block(j)] = (middle[:, block(j)].astype(f32) + feed).astype(bf)

    arrive(0)
    lower(0)
    fold_core(0)
    forward(1, outer)
    forward(2, None)
    arrive(1)
    lower(1)
    fold_core(1)
    forward(3, None)
    fold_x(0)
    arrive(2)
    lower(2)
    fold_core(2)
    fold_x(1)
    arrive(3)
    lower(3)
    fold_core(3)
    fold_x(2)
    fold_side(1)
    fold_side(0)
    fold_x(3)
    fold_side(2)
    fold_side(3)
    for i in range(n):
        finish(i)
    for copy, when in sent:
        if when is None:
            copy.wait_send()
        else:
            pl.when(when)(copy.wait_send)


def spread_columns(heads):
    head = QUERY_KEY_PLAIN + QUERY_KEY_ROTARY
    half = QUERY_KEY_ROTARY // 2
    unit = QUERY_KEY_PLAIN + VALUE_HEAD_SIZE
    lanes = heads * QUERY_KEY_ROTARY
    perm = np.zeros((heads * head, heads * unit + 2 * lanes), np.float32)
    turn = np.zeros((QUERY_KEY_ROTARY, 2 * lanes), np.float32)
    for h in range(heads):
        for r in range(QUERY_KEY_PLAIN):
            perm[h * head + r, h * unit + r] = 1.0
        for r in range(QUERY_KEY_ROTARY):
            col = h * QUERY_KEY_ROTARY + r
            other, sign = (r + half, -1.0) if r < half else (r - half, 1.0)
            turn[r, col] = 1.0
            turn[other, lanes + col] = sign
            perm[h * head + QUERY_KEY_PLAIN + r, heads * unit + col] = 1.0
            perm[h * head + QUERY_KEY_PLAIN + other, heads * unit + lanes + col] = sign
    return jnp.asarray(perm, jnp.bfloat16), jnp.asarray(turn, jnp.bfloat16)


def run_layer(
    hidden_in, query_latent_rows, key_value_latent, rotary_key, query_norm_gain, key_value_gain,
    query_up_weight, key_value_up_weight, out_proj, feed_gain, feed_up, feed_down, position,
):
    n = lax.axis_size("sp")
    rows, width = hidden_in.shape
    heads = query_up_weight.shape[1] // (QUERY_KEY_PLAIN + QUERY_KEY_ROTARY)
    share = rows // lax.axis_size("tp")
    hid = feed_up.shape[1] // n
    unit = QUERY_KEY_PLAIN + VALUE_HEAD_SIZE
    lanes = heads * QUERY_KEY_ROTARY
    rank = key_value_latent.shape[1]
    bf = jnp.bfloat16
    half = QUERY_KEY_ROTARY // 2
    inverse = 10000.0 ** (-jnp.arange(half, dtype=jnp.float32) * 2.0 / QUERY_KEY_ROTARY)
    angles = position[:, None] * jnp.tile(inverse, lanes // half)[None, :]
    table = jnp.stack([jnp.cos(angles), jnp.sin(angles)])
    perm, turn = spread_columns(heads)
    vmem = pl.BlockSpec(memory_space=pltpu.VMEM)
    anywhere = pl.BlockSpec(memory_space=pl.ANY)
    wide = width // n
    copies = 32 * n
    block = (share, width)
    return pl.pallas_call(
        lambda *refs: layer_kernel(heads, *refs),
        out_shape=jax.ShapeDtypeStruct(block, bf),
        in_specs=[vmem] + [anywhere] * 3 + [vmem] * 4 + [anywhere] * 7,
        out_specs=vmem,
        scratch_shapes=[
            pltpu.VMEM(key_value_latent.shape, bf),
            pltpu.VMEM(rotary_key.shape, bf),
            pltpu.VMEM(query_latent_rows.shape, bf),
            pltpu.VMEM(query_up_weight.shape, bf),
            pltpu.VMEM(key_value_up_weight.shape, bf),
            pltpu.VMEM(perm.shape, bf),
            pltpu.VMEM(block, bf),
            pltpu.VMEM((n, 2, 2, share, rank + lanes), bf),
            pltpu.VMEM((heads, n * rows, unit + lanes), bf),
            pltpu.VMEM((heads, rows, unit + lanes), bf),
            pltpu.VMEM((2, *out_proj.shape), bf),
            pltpu.VMEM((heads // 2, rows, unit), bf),
            pltpu.VMEM((2, share, out_proj.shape[0] * 2), bf),
            pltpu.VMEM((n, share, wide), bf),
            pltpu.VMEM((n, share, wide), bf),
            pltpu.VMEM((feed_up.shape[0] * n, hid), bf),
            pltpu.VMEM((hid, width), bf),
            pltpu.VMEM(block, bf),
            pltpu.VMEM((n, 2, 2, *block), bf),
            pltpu.VMEM((n, rows, hid), bf),
            pltpu.VMEM((n, 2, n, 2, share, wide), bf),
            pltpu.VMEM((n, n, 2, share, wide), bf),
            pltpu.VMEM((n, n, share, wide), bf),
            pltpu.VMEM((n, n, share, wide), bf),
            pltpu.VMEM((n, n, share, wide), bf),
            pltpu.VMEM((n, 3, share, wide), bf),
            pltpu.VMEM((n, 2, share, wide), bf),
            pltpu.VMEM((n, share, wide), bf),
            pltpu.SemaphoreType.DMA((copies,)),
            pltpu.SemaphoreType.DMA((copies,)),
            pltpu.SemaphoreType.DMA((16,)),
        ],
        compiler_params=pltpu.CompilerParams(
            collective_id=0, has_side_effects=True, vmem_limit_bytes=60 * 1024 * 1024
        ),
    )(
        table, key_value_latent, rotary_key, query_latent_rows,
        query_norm_gain.reshape(1, -1), key_value_gain.reshape(1, -1), feed_gain.reshape(1, -1), turn,
        perm, query_up_weight, key_value_up_weight, hidden_in, out_proj, feed_up, feed_down,
    )


def fits_kernel(tokens, query_up_weight, feed_up):
    n = lax.axis_size("sp")
    hid = feed_up.shape[1] // n
    heads = query_up_weight.shape[1] // (QUERY_KEY_PLAIN + QUERY_KEY_ROTARY)
    return (
        lax.axis_size("grp") == 2
        and lax.axis_size("tp") == 4
        and n == 4
        and tokens * n <= 1024
        and tokens % 64 == 0
        and hid % 128 == 0
        and hid <= 512
        and heads * QUERY_KEY_ROTARY == 128
    )


def on_device(
    hidden_in,
    query_latent_rows,
    key_value_latent,
    rotary_key,
    query_norm_gain,
    key_value_gain,
    query_up_weight,
    key_value_up_weight,
    out_proj,
    feed_gain,
    feed_up,
    feed_down,
):
    tokens_here = hidden_in.shape[0]
    heads_here = query_up_weight.shape[1] // (QUERY_KEY_PLAIN + QUERY_KEY_ROTARY)
    position = (lax.axis_index("sp") * tokens_here + jnp.arange(tokens_here)).astype(jnp.float32)
    if fits_kernel(tokens_here, query_up_weight, feed_up):
        return run_layer(
            hidden_in, query_latent_rows, key_value_latent, rotary_key, query_norm_gain,
            key_value_gain, query_up_weight, key_value_up_weight, out_proj, feed_gain, feed_up,
            feed_down, position,
        )
    scale_factor = (QUERY_KEY_PLAIN + QUERY_KEY_ROTARY) ** (-0.5)
    query_norm = normalize(query_latent_rows, query_norm_gain).astype(jnp.bfloat16)
    queries = jnp.dot(query_norm, query_up_weight, preferred_element_type=jnp.float32).reshape(
        tokens_here, heads_here, QUERY_KEY_PLAIN + QUERY_KEY_ROTARY
    )
    queries = jnp.concatenate(
        [queries[..., :QUERY_KEY_PLAIN], rotate(queries[..., QUERY_KEY_PLAIN:], position)], axis=-1
    ).astype(jnp.bfloat16)
    query_plain = queries[..., :QUERY_KEY_PLAIN]
    query_turned = queries[..., QUERY_KEY_PLAIN:]
    latent = normalize(key_value_latent, key_value_gain).astype(jnp.bfloat16)
    key_rope = rotate(rotary_key.astype(jnp.float32), position).astype(jnp.bfloat16)

    def attend_block(carry, key_plain, value_rows, rope_rows):
        row_max, denom, accum = carry
        scores = jnp.einsum(
            "qhd,khd->hqk", query_plain, key_plain, preferred_element_type=jnp.float32
        )
        scores = scores + jnp.einsum(
            "qhd,kd->hqk", query_turned, rope_rows, preferred_element_type=jnp.float32
        )
        scores = scores * scale_factor
        new_max = jnp.maximum(row_max, jnp.max(scores, axis=-1))
        expo = jnp.exp(scores - new_max[:, :, None])
        factor = jnp.exp(row_max - new_max)
        denom = denom * factor + jnp.sum(expo, axis=-1)
        update = jnp.einsum(
            "hqk,khd->qhd",
            expo.astype(jnp.bfloat16),
            value_rows,
            preferred_element_type=jnp.float32,
        )
        accum = accum * jnp.transpose(factor)[:, :, None] + update
        return (new_max, denom, accum)

    start_carry = (
        jnp.full((heads_here, tokens_here), -1e30, jnp.float32),
        jnp.zeros((heads_here, tokens_here), jnp.float32),
        jnp.zeros((tokens_here, heads_here, VALUE_HEAD_SIZE), jnp.float32),
    )
    own_keys = jnp.dot(latent, key_value_up_weight, preferred_element_type=jnp.float32).astype(
        jnp.bfloat16
    )
    pieces = (
        lax.all_gather(own_keys, "sp", axis=0, tiled=True),
        lax.all_gather(key_rope, "sp", axis=0, tiled=True),
    )
    rows_in = pieces[0].shape[0]
    block = math.gcd(rows_in, 1024)

    def step_block(index, inner):
        first = index * block
        bulk = lax.dynamic_slice_in_dim(pieces[0], first, block, 0)
        rope_rows = lax.dynamic_slice_in_dim(pieces[1], first, block, 0)
        bulk = bulk.reshape(block, heads_here, QUERY_KEY_PLAIN + VALUE_HEAD_SIZE)
        return attend_block(
            inner, bulk[..., :QUERY_KEY_PLAIN], bulk[..., QUERY_KEY_PLAIN:], rope_rows
        )

    final_carry = lax.fori_loop(0, rows_in // block, step_block, start_carry)
    denom = final_carry[1]
    accum = final_carry[2]
    mixed = (
        (accum / jnp.transpose(denom)[:, :, None])
        .astype(jnp.bfloat16)
        .reshape(tokens_here, heads_here * VALUE_HEAD_SIZE)
    )
    up_own = lax.all_to_all(feed_up, "sp", split_axis=1, concat_axis=0, tiled=True)
    down_own = lax.all_to_all(feed_down, "sp", split_axis=0, concat_axis=1, tiled=True)
    share = tokens_here // lax.axis_size("tp")
    lead = lax.axis_index("tp") * share
    branch = lax.psum_scatter(
        jnp.dot(mixed, out_proj, preferred_element_type=jnp.float32).astype(jnp.bfloat16),
        "tp",
        scatter_dimension=0,
        tiled=True,
    ).astype(jnp.float32)
    hidden_own = lax.dynamic_slice_in_dim(hidden_in, lead, share, 0)
    middle_own = (hidden_own.astype(jnp.float32) + branch).astype(jnp.bfloat16)
    normed_own = normalize(middle_own, feed_gain).astype(jnp.bfloat16)
    normed = lax.all_gather(normed_own, ("sp", "tp"), axis=0, tiled=True)
    upward = jnp.dot(normed, up_own, preferred_element_type=jnp.float32)
    activated = jnp.square(jax.nn.relu(upward)).astype(jnp.bfloat16)
    partial_sum = jnp.dot(activated, down_own, preferred_element_type=jnp.float32)
    feed = lax.psum_scatter(
        partial_sum.astype(jnp.bfloat16), ("sp", "tp"), scatter_dimension=0, tiled=True
    ).astype(jnp.float32)
    return (middle_own.astype(jnp.float32) + feed).astype(jnp.bfloat16)


def solution(mesh):
    return jax.shard_map(
        on_device,
        mesh=mesh,
        in_specs=(
            P(("grp", "sp"), None),
            P(("grp", "sp"), None),
            P(("grp", "sp"), None),
            P(("grp", "sp"), None),
            P(),
            P(),
            P(None, "tp"),
            P(None, "tp"),
            P("tp", None),
            P(),
            P("sp", "tp"),
            P("tp", "sp"),
        ),
        out_specs=P(("grp", "sp", "tp"), None),
        check_vma=False,
    )
```

```python
import math

import jax
import jax.numpy as jnp
import numpy as np
from jax import lax
from jax.experimental import pallas as pl
from jax.experimental.pallas import tpu as pltpu
from jax.sharding import PartitionSpec as P

QUERY_KEY_PLAIN = 64
QUERY_KEY_ROTARY = 32
VALUE_HEAD_SIZE = 64


def normalize(values, gain):
    floats = values.astype(jnp.float32)
    return floats * lax.rsqrt(jnp.mean(floats * floats, axis=-1, keepdims=True) + 1e-06) * gain


def rotate(values, position):
    half_size = values.shape[-1] // 2
    inverse = 10000.0 ** (-jnp.arange(half_size, dtype=jnp.float32) * 2.0 / values.shape[-1])
    angles = position[:, None] * inverse[None, :]
    cosine = jnp.concatenate([jnp.cos(angles), jnp.cos(angles)], axis=-1)
    sine = jnp.concatenate([jnp.sin(angles), jnp.sin(angles)], axis=-1)
    shape = (values.shape[0],) + (1,) * (values.ndim - 2) + (values.shape[-1],)
    turned = jnp.concatenate([-values[..., half_size:], values[..., :half_size]], axis=-1)
    return values * cosine.reshape(shape) + turned * sine.reshape(shape)


MESH = pl.DeviceIdType.MESH


def layer_kernel(
    heads, inverse, turn, kvlat, rk, qlat, gain_q, gain_kv, gain_f, perm, wq, wkv, hidden, op, up, down, out,
    table, spun, gq, gkv, gain, lat_in, rk_in, q_in, wq_in, wkv_in, perm_in, hid_in,
    lat_all, kv_all, q_all, op_chip, mixed, mixed_in, branch_out, branch_in, up_all, down_all, middle,
    norm_all, act, part, rf1, c2, rf2, c3, near_in, cross_out, cross_in, ss, rs, ls,
):
    n = 4
    g, me, t = lax.axis_index("grp"), lax.axis_index("sp"), lax.axis_index("tp")
    c, x = lax.rem(t, 2), t // 2
    share, width = middle.shape
    rows = share * 4
    rank = wkv.shape[0]
    piece_k = up.shape[0]
    hid = down_all.shape[0]
    half_k, half_h = piece_k // 2, hid // 2
    wide = down.shape[1]
    bf, f32 = jnp.bfloat16, jnp.float32
    vh = VALUE_HEAD_SIZE
    unit = QUERY_KEY_PLAIN + vh
    lanes = heads * QUERY_KEY_ROTARY
    scale_factor = (QUERY_KEY_PLAIN + QUERY_KEY_ROTARY) ** (-0.5)
    side = me // 2
    outer = (me == 0) | (me == n - 1)
    inner = (me == 1) | (me == n - 2)
    away = 1 - 2 * side
    partner = me + 1 - 2 * lax.rem(me, 2)
    edge, gate = side * (n - 1), 1 + side
    far_edge, far_gate = (1 - side) * (n - 1), 2 - side

    def near(i):
        if i == 0:
            return me
        if i == 1:
            return partner
        return far_gate if i == 2 else far_edge

    def at_tp(cc, xx):
        return {"tp": xx * 2 + cc}

    sib, xpeer, ypeer = at_tp(1 - c, x), at_tp(c, 1 - x), {"grp": 1 - g}
    barrier = pltpu.get_barrier_semaphore()
    for i in range(1, n):
        pl.semaphore_signal(barrier, inc=1, device_id={"sp": near(i)}, device_id_type=MESH)
    for peer in (sib, xpeer, ypeer):
        pl.semaphore_signal(barrier, inc=1, device_id=peer, device_id_type=MESH)

    def rows_of(tt):
        return pl.ds(pl.multiple_of(tt * share, share), share)

    local = []

    def fetch(src, dst):
        copy = pltpu.make_async_copy(src, dst, ls.at[len(local)])
        copy.start()
        local.append(copy)
        return copy

    got_lat = fetch(kvlat, lat_in)
    got_rk = fetch(rk, rk_in)
    got_gkv = fetch(gain_kv, gkv)
    got_gq = fetch(gain_q, gq)
    got_gain = fetch(gain_f, gain)
    got_perm = fetch(perm, perm_in)
    got_wq = fetch(wq, wq_in)
    got_q = fetch(qlat, q_in)
    got_wkv = fetch(wkv, wkv_in)
    got_op = fetch(op, op_chip.at[c])
    got_hid = fetch(hidden.at[rows_of(t)], hid_in)
    got_up = fetch(
        up.at[:, pl.ds(pl.multiple_of(me * hid, hid), hid)],
        up_all.at[pl.ds(pl.multiple_of(me * piece_k, piece_k), piece_k)],
    )
    got_down = fetch(
        down.at[pl.ds(pl.multiple_of(me * hid, hid), hid)],
        down_all.at[:, pl.ds(pl.multiple_of(me * wide, wide), wide)],
    )

    names = {}
    sent = []

    def slot(name, at):
        if name not in names:
            names[name] = sum(size for _, size in names.values()), 1 if at is None else n
        return names[name][0] + (0 if at is None else at)

    def send(name, src, dst, dev, to=None, by=None, when=None, into=None):
        copy = pltpu.make_async_remote_copy(
            src_ref=src, dst_ref=dst, send_sem=ss.at[slot(name, to)], recv_sem=rs.at[slot(into or name, by)],
            device_id=dev, device_id_type=MESH,
        )
        if when is None:
            copy.start()
        else:
            pl.when(when)(copy.start)
        sent.append((copy, when))

    def land(name, dst, by=None):
        pltpu.make_async_remote_copy(
            src_ref=dst, dst_ref=dst, send_sem=ss.at[slot(name, by)], recv_sem=rs.at[slot(name, by)],
            device_id=sib, device_id_type=MESH,
        ).wait_recv()

    def up_half(owner, hv):
        return up_all.at[pl.ds(pl.multiple_of(owner * piece_k + hv * half_k, half_k), half_k)]

    part_h = half_h // 2

    def down_half(owner, hv, q):
        return down_all.at[
            pl.ds(pl.multiple_of(hv * half_h + q * part_h, part_h), part_h),
            pl.ds(pl.multiple_of(owner * wide, wide), wide),
        ]

    def strip(buf, z, cc, xx, tag):
        if tag[1:] == "":
            return buf.at[z, cc, xx]
        deep = share // 2
        return buf.at[z, cc, xx, int(tag[1:]) * deep : (int(tag[1:]) + 1) * deep]

    def share_on(tag, buf, i):
        z = near(i)
        piece = strip(buf, z, c, x, tag)
        send((tag, "x"), piece, piece, xpeer, z, z)
        send((tag, "s"), piece, piece, sib, z, z)

    def cross_one(tag, buf, i):
        z = near(i)
        piece = strip(buf, z, c, 1 - x, tag)
        land((tag, "x"), piece, z)
        send((tag, "t"), piece, piece, sib, z, z)

    def tags(tag):
        return ("n0", "n1") if tag == "n" else (tag,)

    def cross(tag, buf, i):
        for one in tags(tag):
            cross_one(one, buf, i)

    def land_sib(tag, buf, i):
        for one in tags(tag):
            land((one, "s"), strip(buf, near(i), 1 - c, x, one), near(i))

    def settle(tag, buf, i, both=True):
        z = near(i)
        if both:
            land_sib(tag, buf, i)
        for one in tags(tag):
            land((one, "t"), strip(buf, z, 1 - c, 1 - x, one), z)

    def make_latent(cc, xx):
        here = rows_of(xx * 2 + cc)
        lat_all[me, cc, xx, :, :rank] = normalize(lat_in[here, :], gkv[...].reshape(1, -1)).astype(bf)
        lat_all[me, cc, xx, :, rank:] = (
            spun[here, :lanes] * table[0, here, :] + spun[here, lanes:] * table[1, here, :]
        ).astype(bf)

    def make_table(tt):
        here = rows_of(tt)
        place = lax.broadcasted_iota(jnp.int32, (share, lanes), 0) + (me * rows + tt * share)
        angle = place.astype(f32) * inverse[...]
        table[0, here, :] = jnp.cos(angle)
        table[1, here, :] = jnp.sin(angle)

    make_table(t)
    got_rk.wait()
    spun[...] = lax.dot_general(
        rk_in[...], turn[...], (((0,), (0,)), ((), ())), preferred_element_type=f32
    )
    got_lat.wait()
    got_gkv.wait()
    make_latent(c, x)
    pl.semaphore_wait(barrier, n + 2)
    own = lat_all.at[me, c, x]
    for i in reversed(range(1, n)):
        send(("l", "z"), own, own, {"sp": near(i)}, near(i), me)
    got_op.wait()
    send("os", op_chip.at[c], op_chip.at[c], sib)
    for cc, xx in ((1 - c, x), (c, 1 - x), (1 - c, 1 - x)):
        make_table(xx * 2 + cc)
        make_latent(cc, xx)
    got_perm.wait()
    got_wq.wait()
    wide_q = jnp.dot(wq_in[...], perm_in[...], preferred_element_type=f32).astype(bf)
    got_q.wait()
    got_gq.wait()
    query_norm = normalize(q_in[...], gq[...].reshape(1, -1)).astype(bf)
    spread = jnp.dot(query_norm, wide_q, preferred_element_type=f32)
    first = heads * unit
    spin = (
        spread[:, first : first + lanes] * table[0] + spread[:, first + lanes : first + 2 * lanes] * table[1]
    )
    lane = lax.broadcasted_iota(jnp.int32, (rows, lanes), 1)
    for h in range(heads):
        q_all[h, :, :unit] = spread[:, h * unit : (h + 1) * unit].astype(bf)
        keep = (lane >= h * QUERY_KEY_ROTARY) & (lane < (h + 1) * QUERY_KEY_ROTARY)
        q_all[h, :, unit:] = jnp.where(keep, spin, 0.0).astype(bf)

    land(("l", "z"), lat_all.at[near(1), c, x], near(1))
    share_on("l", lat_all, 1)
    land(("l", "z"), lat_all.at[near(2), c, x], near(2))
    share_on("l", lat_all, 2)
    land(("l", "z"), lat_all.at[near(3), c, x], near(3))
    share_on("l", lat_all, 3)
    def send_up(i, when):
        send(
            "up",
            up.at[
                pl.ds(pl.multiple_of(g * half_k, half_k), half_k),
                pl.ds(pl.multiple_of(near(i) * hid, hid), hid),
            ],
            up_half(me, g),
            {"sp": near(i)},
            near(i),
            me,
            when,
        )

    send_up(3, inner)
    send_up(1, None)
    got_wkv.wait()
    for i in range(1, n):
        cross("l", lat_all, i)
    send_up(3, outer)
    send_up(2, outer)
    for i in range(1, n):
        settle("l", lat_all, i)
    for j in range(n):
        made = jnp.dot(
            lat_all[j, :, :, :, :rank].reshape(rows, rank), wkv_in[...], preferred_element_type=f32
        ).astype(bf)
        rope = lat_all[j, :, :, :, rank:].reshape(rows, lanes)
        for h in range(heads):
            kv_all[h, j * rows : (j + 1) * rows, :unit] = made[:, h * unit : (h + 1) * unit]
            kv_all[h, j * rows : (j + 1) * rows, unit:] = rope

    contract = (((1,), (1,)), ((), ()))
    low = lax.broadcasted_iota(jnp.int32, (rows, unit), 1) < vh

    def attend(h):
        scores = lax.dot_general(q_all[h], kv_all[h], contract, preferred_element_type=f32)
        scores = scores * scale_factor
        expo = jnp.exp(scores - jnp.max(scores, axis=-1, keepdims=True))
        total = jnp.sum(expo, axis=-1, keepdims=True)
        mix = jnp.dot(expo.astype(bf), kv_all[h, :, :unit], preferred_element_type=f32)
        return mix / total

    def head_cols(cc, p):
        return pl.ds(pl.multiple_of(cc * heads * vh + p * unit, unit), unit)

    for p in range(heads // 2):
        left, right = attend(2 * p), attend(2 * p + 1)
        pair = jnp.where(low, pltpu.roll(left, vh, 1), right)
        mixed[p] = pair.astype(bf)
        for xx in range(2):
            send(
                ("m", p, xx), mixed.at[p, rows_of(xx * 2 + 1 - c)], mixed_in.at[xx, :, head_cols(c, p)], sib
            )
            mixed_in[xx, :, head_cols(c, p)] = mixed[p, rows_of(xx * 2 + c), :]

    land("os", op_chip.at[1 - c])
    for p in range(heads // 2):
        for xx in range(2):
            land(("m", p, xx), mixed_in.at[xx, :, head_cols(1 - c, p)])

    tiles = width // wide
    chip_heads = 2 * heads * vh

    def project(xx, j):
        return jnp.dot(
            mixed_in[xx],
            op_chip[:, :, j * wide : (j + 1) * wide].reshape(chip_heads, wide),
            preferred_element_type=f32,
        )

    for j in range(tiles):
        branch_out[j] = project(1 - x, j).astype(bf)
        send(("b", j), branch_out.at[j], branch_in.at[j], xpeer)
    got_hid.wait()
    for j in range(tiles):
        kept = project(x, j)
        land(("b", j), branch_in.at[j])
        cols = slice(j * wide, (j + 1) * wide)
        middle[:, cols] = (hid_in[:, cols].astype(f32) + (kept + branch_in[j].astype(f32))).astype(bf)
    got_gain.wait()
    norm_all[me, c, x] = normalize(middle[...], gain[...].reshape(1, -1)).astype(bf)

    def pass_on(i, to, when, one):
        z = near(i)
        piece = strip(norm_all, z, c, x, one)
        send((one, "z"), piece, piece, {"sp": to}, z, z, when)

    def send_down(i, when):
        for q in range(2):
            send(
                ("dn", q),
                down.at[pl.ds(pl.multiple_of(near(i) * hid + g * half_h + q * part_h, part_h), part_h)],
                down_half(me, g, q),
                {"sp": near(i)},
                near(i),
                me,
                when,
            )

    for one in tags("n"):
        own = strip(norm_all, me, c, x, one)
        send((one, "z"), own, own, {"sp": partner}, me, me)
        send((one, "c"), own, own, {"sp": far_gate}, None, me, inner, (one, "z"))
        share_on(one, norm_all, 0)
    send_down(1, outer)
    def forward_up(i, when):
        piece = up_half(near(i), g)
        if when is None:
            land("up", piece, near(i))
        else:
            pl.when(when)(lambda: land("up", piece, near(i)))
        send("uy", piece, piece, ypeer, near(i), near(i), when)

    forward_up(1, None)
    forward_up(2, outer)
    forward_up(3, None)

    def raise_block(i):
        z = near(i)
        upward = jnp.dot(norm_all[z].reshape(rows, width), up_all[...], preferred_element_type=f32)
        act[z] = jnp.square(jnp.maximum(upward, 0.0)).astype(bf)

    def relay(i, to):
        for one in tags("n"):
            land((one, "z"), strip(norm_all, near(i), c, x, one), near(i))
            pass_on(i, to, inner, one)
            share_on(one, norm_all, i)

    def forward(i, when):
        j = near(i)
        for q in range(2):
            piece = down_half(j, g, q)
            if when is None:
                land(("dn", q), piece, j)
            else:
                pl.when(when)(lambda: land(("dn", q), piece, j))
            send(("dy", q), piece, piece, ypeer, j, j, when)

    relay(1, far_gate)
    send_up(2, inner)
    cross("n", norm_all, 0)
    relay(2, partner)
    cross("n", norm_all, 1)
    relay(3, partner)
    land_sib("n", norm_all, 3)
    send_down(2, inner)
    send_down(3, outer)
    send_down(2, outer)
    forward_up(2, inner)
    cross("n", norm_all, 2)
    send_down(3, inner)
    send_down(1, inner)
    for i in range(1, n):
        land("uy", up_half(near(i), 1 - g), near(i))
    got_up.wait()
    settle("n", norm_all, 0)
    raise_block(0)
    cross("n", norm_all, 3)
    settle("n", norm_all, 1)
    raise_block(1)
    settle("n", norm_all, 2)
    raise_block(2)
    forward(1, inner)
    settle("n", norm_all, 3, False)
    raise_block(3)

    def block(j):
        return pl.ds(pl.multiple_of(j * wide, wide), wide)

    def arrive(i):
        if i:
            for q in range(2):
                land(("dy", q), down_half(near(i), 1 - g, q), near(i))
        else:
            got_down.wait()

    def lower(i):
        j = near(i)

        @pl.loop(0, n)
        def _(d):
            made = jnp.dot(act[d], down_all[:, block(j)], preferred_element_type=f32)
            made = made.astype(bf).reshape(2, 2, share, wide)
            part[j, 0, d] = made[0]
            part[j, 1, d] = made[1]

        send("f1", part.at[j, 1 - c], rf1.at[j], sib, j, j)

    def fold_core(i):
        j = near(i)
        land("f1", rf1.at[j], j)
        c2[j] = (part[j, c, :, 1 - x].astype(f32) + rf1[j, :, 1 - x].astype(f32)).astype(bf)
        send("f2", c2.at[j], rf2.at[j], xpeer, j, j)

    def fold_x(i):
        j = near(i)
        land("f2", rf2.at[j], j)
        c3[j] = (
            part[j, c, :, x].astype(f32) + rf1[j, :, x].astype(f32) + rf2[j].astype(f32)
        ).astype(bf)
        send("pe", c3.at[j, far_edge], near_in.at[j, 2], {"sp": partner}, j, j, outer)
        send("pg", c3.at[j, far_gate], near_in.at[j, 1], {"sp": partner}, j, j, outer)
        send("p", c3.at[j, partner], near_in.at[j, 0], {"sp": partner}, j, j)

    def fold_side(i):
        j = near(i)

        @pl.when(inner)
        def _():
            land("pe", near_in.at[j, 2], j)
            cross_out[j, 1] = (c3[j, far_edge].astype(f32) + near_in[j, 2].astype(f32)).astype(bf)

        send("q1", cross_out.at[j, 1], cross_in.at[j], {"sp": far_edge}, j, j, inner, "q0")

        @pl.when(inner)
        def _():
            land("pg", near_in.at[j, 1], j)
            cross_out[j, 0] = (c3[j, far_gate].astype(f32) + near_in[j, 1].astype(f32)).astype(bf)

        send("q0", cross_out.at[j, 0], cross_in.at[j], {"sp": far_gate}, j, j, inner)

    def finish(i):
        j = near(i)
        land("p", near_in.at[j, 0], j)
        land("q0", cross_in.at[j], j)
        feed = c3[j, me].astype(f32) + near_in[j, 0].astype(f32) + cross_in[j].astype(f32)
        out[:, block(j)] = (middle[:, block(j)].astype(f32) + feed).astype(bf)

    arrive(0)
    lower(0)
    fold_core(0)
    forward(1, outer)
    forward(2, None)
    arrive(1)
    lower(1)
    fold_core(1)
    forward(3, None)
    fold_x(0)
    arrive(2)
    lower(2)
    fold_core(2)
    fold_x(1)
    arrive(3)
    lower(3)
    fold_core(3)
    fold_x(2)
    fold_side(1)
    fold_side(0)
    fold_x(3)
    fold_side(2)
    fold_side(3)
    for i in range(n):
        finish(i)
    for copy, when in sent:
        if when is None:
            copy.wait_send()
        else:
            pl.when(when)(copy.wait_send)


def spread_columns(heads):
    head = QUERY_KEY_PLAIN + QUERY_KEY_ROTARY
    half = QUERY_KEY_ROTARY // 2
    unit = QUERY_KEY_PLAIN + VALUE_HEAD_SIZE
    lanes = heads * QUERY_KEY_ROTARY
    perm = np.zeros((heads * head, heads * unit + 2 * lanes), np.float32)
    turn = np.zeros((QUERY_KEY_ROTARY, 2 * lanes), np.float32)
    for h in range(heads):
        for r in range(QUERY_KEY_PLAIN):
            perm[h * head + r, h * unit + r] = 1.0
        for r in range(QUERY_KEY_ROTARY):
            col = h * QUERY_KEY_ROTARY + r
            other, sign = (r + half, -1.0) if r < half else (r - half, 1.0)
            turn[r, col] = 1.0
            turn[other, lanes + col] = sign
            perm[h * head + QUERY_KEY_PLAIN + r, heads * unit + col] = 1.0
            perm[h * head + QUERY_KEY_PLAIN + other, heads * unit + lanes + col] = sign
    return jnp.asarray(perm, jnp.bfloat16), jnp.asarray(turn, jnp.bfloat16)


def run_layer(
    hidden_in, query_latent_rows, key_value_latent, rotary_key, query_norm_gain, key_value_gain,
    query_up_weight, key_value_up_weight, out_proj, feed_gain, feed_up, feed_down, position,
):
    n = lax.axis_size("sp")
    rows, width = hidden_in.shape
    heads = query_up_weight.shape[1] // (QUERY_KEY_PLAIN + QUERY_KEY_ROTARY)
    share = rows // lax.axis_size("tp")
    hid = feed_up.shape[1] // n
    unit = QUERY_KEY_PLAIN + VALUE_HEAD_SIZE
    lanes = heads * QUERY_KEY_ROTARY
    rank = key_value_latent.shape[1]
    bf = jnp.bfloat16
    half = QUERY_KEY_ROTARY // 2
    inverse = 10000.0 ** (-np.arange(half, dtype=np.float32) * 2.0 / QUERY_KEY_ROTARY)
    inverse = jnp.asarray(np.tile(inverse, lanes // half)[None, :], jnp.float32)
    perm, turn = spread_columns(heads)
    vmem = pl.BlockSpec(memory_space=pltpu.VMEM)
    anywhere = pl.BlockSpec(memory_space=pl.ANY)
    wide = width // n
    copies = 28 * n
    block = (share, width)
    return pl.pallas_call(
        lambda *refs: layer_kernel(heads, *refs),
        out_shape=pltpu.VMEM(block, bf),
        in_specs=[vmem] * 2 + [anywhere] * 13,
        out_specs=vmem,
        scratch_shapes=[
            pltpu.VMEM((2, rows, lanes), jnp.float32),
            pltpu.VMEM((rows, 2 * lanes), jnp.float32),
            pltpu.VMEM(query_norm_gain.shape, jnp.float32),
            pltpu.VMEM(key_value_gain.shape, jnp.float32),
            pltpu.VMEM(feed_gain.shape, jnp.float32),
            pltpu.VMEM(key_value_latent.shape, bf),
            pltpu.VMEM(rotary_key.T.shape, bf),
            pltpu.VMEM(query_latent_rows.shape, bf),
            pltpu.VMEM(query_up_weight.shape, bf),
            pltpu.VMEM(key_value_up_weight.shape, bf),
            pltpu.VMEM(perm.shape, bf),
            pltpu.VMEM(block, bf),
            pltpu.VMEM((n, 2, 2, share, rank + lanes), bf),
            pltpu.VMEM((heads, n * rows, unit + lanes), bf),
            pltpu.VMEM((heads, rows, unit + lanes), bf),
            pltpu.VMEM((2, *out_proj.shape), bf),
            pltpu.VMEM((heads // 2, rows, unit), bf),
            pltpu.VMEM((2, share, out_proj.shape[0] * 2), bf),
            pltpu.VMEM((n, share, wide), bf),
            pltpu.VMEM((n, share, wide), bf),
            pltpu.VMEM((feed_up.shape[0] * n, hid), bf),
            pltpu.VMEM((hid, width), bf),
            pltpu.VMEM(block, bf),
            pltpu.VMEM((n, 2, 2, *block), bf),
            pltpu.VMEM((n, rows, hid), bf),
            pltpu.VMEM((n, 2, n, 2, share, wide), bf),
            pltpu.VMEM((n, n, 2, share, wide), bf),
            pltpu.VMEM((n, n, share, wide), bf),
            pltpu.VMEM((n, n, share, wide), bf),
            pltpu.VMEM((n, n, share, wide), bf),
            pltpu.VMEM((n, 3, share, wide), bf),
            pltpu.VMEM((n, 2, share, wide), bf),
            pltpu.VMEM((n, share, wide), bf),
            pltpu.SemaphoreType.DMA((copies,)),
            pltpu.SemaphoreType.DMA((copies,)),
            pltpu.SemaphoreType.DMA((16,)),
        ],
        compiler_params=pltpu.CompilerParams(
            collective_id=0, has_side_effects=True, vmem_limit_bytes=60 * 1024 * 1024
        ),
    )(
        inverse, turn, key_value_latent, rotary_key.T, query_latent_rows, query_norm_gain,
        key_value_gain, feed_gain, perm, query_up_weight, key_value_up_weight, hidden_in, out_proj,
        feed_up, feed_down,
    )


def fits_kernel(tokens, query_up_weight, feed_up):
    n = lax.axis_size("sp")
    hid = feed_up.shape[1] // n
    heads = query_up_weight.shape[1] // (QUERY_KEY_PLAIN + QUERY_KEY_ROTARY)
    return (
        lax.axis_size("grp") == 2
        and lax.axis_size("tp") == 4
        and n == 4
        and tokens * n <= 1024
        and tokens % 64 == 0
        and hid % 128 == 0
        and hid <= 512
        and heads * QUERY_KEY_ROTARY == 128
    )


def on_device(
    hidden_in,
    query_latent_rows,
    key_value_latent,
    rotary_key,
    query_norm_gain,
    key_value_gain,
    query_up_weight,
    key_value_up_weight,
    out_proj,
    feed_gain,
    feed_up,
    feed_down,
):
    tokens_here = hidden_in.shape[0]
    heads_here = query_up_weight.shape[1] // (QUERY_KEY_PLAIN + QUERY_KEY_ROTARY)
    position = (lax.axis_index("sp") * tokens_here + jnp.arange(tokens_here)).astype(jnp.float32)
    if fits_kernel(tokens_here, query_up_weight, feed_up):
        return run_layer(
            hidden_in, query_latent_rows, key_value_latent, rotary_key, query_norm_gain,
            key_value_gain, query_up_weight, key_value_up_weight, out_proj, feed_gain, feed_up,
            feed_down, position,
        )
    scale_factor = (QUERY_KEY_PLAIN + QUERY_KEY_ROTARY) ** (-0.5)
    query_norm = normalize(query_latent_rows, query_norm_gain).astype(jnp.bfloat16)
    queries = jnp.dot(query_norm, query_up_weight, preferred_element_type=jnp.float32).reshape(
        tokens_here, heads_here, QUERY_KEY_PLAIN + QUERY_KEY_ROTARY
    )
    queries = jnp.concatenate(
        [queries[..., :QUERY_KEY_PLAIN], rotate(queries[..., QUERY_KEY_PLAIN:], position)], axis=-1
    ).astype(jnp.bfloat16)
    query_plain = queries[..., :QUERY_KEY_PLAIN]
    query_turned = queries[..., QUERY_KEY_PLAIN:]
    latent = normalize(key_value_latent, key_value_gain).astype(jnp.bfloat16)
    key_rope = rotate(rotary_key.astype(jnp.float32), position).astype(jnp.bfloat16)

    def attend_block(carry, key_plain, value_rows, rope_rows):
        row_max, denom, accum = carry
        scores = jnp.einsum(
            "qhd,khd->hqk", query_plain, key_plain, preferred_element_type=jnp.float32
        )
        scores = scores + jnp.einsum(
            "qhd,kd->hqk", query_turned, rope_rows, preferred_element_type=jnp.float32
        )
        scores = scores * scale_factor
        new_max = jnp.maximum(row_max, jnp.max(scores, axis=-1))
        expo = jnp.exp(scores - new_max[:, :, None])
        factor = jnp.exp(row_max - new_max)
        denom = denom * factor + jnp.sum(expo, axis=-1)
        update = jnp.einsum(
            "hqk,khd->qhd",
            expo.astype(jnp.bfloat16),
            value_rows,
            preferred_element_type=jnp.float32,
        )
        accum = accum * jnp.transpose(factor)[:, :, None] + update
        return (new_max, denom, accum)

    start_carry = (
        jnp.full((heads_here, tokens_here), -1e30, jnp.float32),
        jnp.zeros((heads_here, tokens_here), jnp.float32),
        jnp.zeros((tokens_here, heads_here, VALUE_HEAD_SIZE), jnp.float32),
    )
    own_keys = jnp.dot(latent, key_value_up_weight, preferred_element_type=jnp.float32).astype(
        jnp.bfloat16
    )
    pieces = (
        lax.all_gather(own_keys, "sp", axis=0, tiled=True),
        lax.all_gather(key_rope, "sp", axis=0, tiled=True),
    )
    rows_in = pieces[0].shape[0]
    block = math.gcd(rows_in, 1024)

    def step_block(index, inner):
        first = index * block
        bulk = lax.dynamic_slice_in_dim(pieces[0], first, block, 0)
        rope_rows = lax.dynamic_slice_in_dim(pieces[1], first, block, 0)
        bulk = bulk.reshape(block, heads_here, QUERY_KEY_PLAIN + VALUE_HEAD_SIZE)
        return attend_block(
            inner, bulk[..., :QUERY_KEY_PLAIN], bulk[..., QUERY_KEY_PLAIN:], rope_rows
        )

    final_carry = lax.fori_loop(0, rows_in // block, step_block, start_carry)
    denom = final_carry[1]
    accum = final_carry[2]
    mixed = (
        (accum / jnp.transpose(denom)[:, :, None])
        .astype(jnp.bfloat16)
        .reshape(tokens_here, heads_here * VALUE_HEAD_SIZE)
    )
    up_own = lax.all_to_all(feed_up, "sp", split_axis=1, concat_axis=0, tiled=True)
    down_own = lax.all_to_all(feed_down, "sp", split_axis=0, concat_axis=1, tiled=True)
    share = tokens_here // lax.axis_size("tp")
    lead = lax.axis_index("tp") * share
    branch = lax.psum_scatter(
        jnp.dot(mixed, out_proj, preferred_element_type=jnp.float32).astype(jnp.bfloat16),
        "tp",
        scatter_dimension=0,
        tiled=True,
    ).astype(jnp.float32)
    hidden_own = lax.dynamic_slice_in_dim(hidden_in, lead, share, 0)
    middle_own = (hidden_own.astype(jnp.float32) + branch).astype(jnp.bfloat16)
    normed_own = normalize(middle_own, feed_gain).astype(jnp.bfloat16)
    normed = lax.all_gather(normed_own, ("sp", "tp"), axis=0, tiled=True)
    upward = jnp.dot(normed, up_own, preferred_element_type=jnp.float32)
    activated = jnp.square(jax.nn.relu(upward)).astype(jnp.bfloat16)
    partial_sum = jnp.dot(activated, down_own, preferred_element_type=jnp.float32)
    feed = lax.psum_scatter(
        partial_sum.astype(jnp.bfloat16), ("sp", "tp"), scatter_dimension=0, tiled=True
    ).astype(jnp.float32)
    return (middle_own.astype(jnp.float32) + feed).astype(jnp.bfloat16)


def solution(mesh):
    return jax.shard_map(
        on_device,
        mesh=mesh,
        in_specs=(
            P(("grp", "sp"), None),
            P(("grp", "sp"), None),
            P(("grp", "sp"), None),
            P(("grp", "sp"), None),
            P(),
            P(),
            P(None, "tp"),
            P(None, "tp"),
            P("tp", None),
            P(),
            P("sp", "tp"),
            P("tp", "sp"),
        ),
        out_specs=P(("grp", "sp", "tp"), None),
        check_vma=False,
    )
```

```python
import math

import jax
import jax.numpy as jnp
import numpy as np
from jax import lax
from jax.experimental import pallas as pl
from jax.experimental.pallas import tpu as pltpu
from jax.sharding import PartitionSpec as P

QUERY_KEY_PLAIN = 64
QUERY_KEY_ROTARY = 32
VALUE_HEAD_SIZE = 64


def normalize(values, gain):
    floats = values.astype(jnp.float32)
    return floats * lax.rsqrt(jnp.mean(floats * floats, axis=-1, keepdims=True) + 1e-06) * gain


def rotate(values, position):
    half_size = values.shape[-1] // 2
    inverse = 10000.0 ** (-jnp.arange(half_size, dtype=jnp.float32) * 2.0 / values.shape[-1])
    angles = position[:, None] * inverse[None, :]
    cosine = jnp.concatenate([jnp.cos(angles), jnp.cos(angles)], axis=-1)
    sine = jnp.concatenate([jnp.sin(angles), jnp.sin(angles)], axis=-1)
    shape = (values.shape[0],) + (1,) * (values.ndim - 2) + (values.shape[-1],)
    turned = jnp.concatenate([-values[..., half_size:], values[..., :half_size]], axis=-1)
    return values * cosine.reshape(shape) + turned * sine.reshape(shape)


MESH = pl.DeviceIdType.MESH


def layer_kernel(
    heads, inverse, turn, kvlat, rk, qlat, gain_q, gain_kv, gain_f, perm, wq, wkv, hidden, op, up, down, out,
    table, spun, gq, gkv, gain, lat_in, rk_in, q_in, wq_in, wkv_in, perm_in, hid_in,
    lat_all, kv_all, q_all, op_chip, mixed, mixed_in, branch_out, branch_in, up_all, down_all, middle,
    norm_all, act, part, rf1, c2, rf2, c3, near_in, cross_out, cross_in, ss, rs, ls,
):
    n = 4
    g, me, t = lax.axis_index("grp"), lax.axis_index("sp"), lax.axis_index("tp")
    c, x = lax.rem(t, 2), t // 2
    share, width = middle.shape
    rows = share * 4
    rank = wkv.shape[0]
    piece_k = up.shape[0]
    hid = down_all.shape[0]
    half_k, half_h = piece_k // 2, hid // 2
    wide = down.shape[1]
    bf, f32 = jnp.bfloat16, jnp.float32
    vh = VALUE_HEAD_SIZE
    unit = QUERY_KEY_PLAIN + vh
    lanes = heads * QUERY_KEY_ROTARY
    scale_factor = (QUERY_KEY_PLAIN + QUERY_KEY_ROTARY) ** (-0.5)
    side = me // 2
    outer = (me == 0) | (me == n - 1)
    inner = (me == 1) | (me == n - 2)
    away = 1 - 2 * side
    partner = me + 1 - 2 * lax.rem(me, 2)
    edge, gate = side * (n - 1), 1 + side
    far_edge, far_gate = (1 - side) * (n - 1), 2 - side

    def near(i):
        if i == 0:
            return me
        if i == 1:
            return partner
        return far_gate if i == 2 else far_edge

    def at_tp(cc, xx):
        return {"tp": xx * 2 + cc}

    sib, xpeer, ypeer = at_tp(1 - c, x), at_tp(c, 1 - x), {"grp": 1 - g}
    barrier = pltpu.get_barrier_semaphore()
    for i in range(1, n):
        pl.semaphore_signal(barrier, inc=1, device_id={"sp": near(i)}, device_id_type=MESH)
    for peer in (sib, xpeer, ypeer):
        pl.semaphore_signal(barrier, inc=1, device_id=peer, device_id_type=MESH)

    def rows_of(tt):
        return pl.ds(pl.multiple_of(tt * share, share), share)

    local = []

    def fetch(src, dst):
        copy = pltpu.make_async_copy(src, dst, ls.at[len(local)])
        copy.start()
        local.append(copy)
        return copy

    got_lat = fetch(kvlat, lat_in)
    got_rk = fetch(rk, rk_in)
    got_gkv = fetch(gain_kv, gkv)
    got_gq = fetch(gain_q, gq)
    got_gain = fetch(gain_f, gain)
    got_perm = fetch(perm, perm_in)
    got_wq = fetch(wq, wq_in)
    got_q = fetch(qlat, q_in)
    got_wkv = fetch(wkv, wkv_in)
    got_op = fetch(op, op_chip.at[c])
    got_hid = fetch(hidden.at[rows_of(t)], hid_in)
    got_up = fetch(
        up.at[:, pl.ds(pl.multiple_of(me * hid, hid), hid)],
        up_all.at[pl.ds(pl.multiple_of(me * piece_k, piece_k), piece_k)],
    )
    got_down = fetch(
        down.at[pl.ds(pl.multiple_of(me * hid, hid), hid)],
        down_all.at[:, pl.ds(pl.multiple_of(me * wide, wide), wide)],
    )

    names = {}
    sent = []

    def slot(name, at):
        if name not in names:
            names[name] = sum(size for _, size in names.values()), 1 if at is None else n
        return names[name][0] + (0 if at is None else at)

    def send(name, src, dst, dev, to=None, by=None, when=None, into=None):
        copy = pltpu.make_async_remote_copy(
            src_ref=src, dst_ref=dst, send_sem=ss.at[slot(name, to)], recv_sem=rs.at[slot(into or name, by)],
            device_id=dev, device_id_type=MESH,
        )
        if when is None:
            copy.start()
        else:
            pl.when(when)(copy.start)
        sent.append((copy, when))

    def land(name, dst, by=None):
        pltpu.make_async_remote_copy(
            src_ref=dst, dst_ref=dst, send_sem=ss.at[slot(name, by)], recv_sem=rs.at[slot(name, by)],
            device_id=sib, device_id_type=MESH,
        ).wait_recv()

    def up_half(owner, hv):
        return up_all.at[pl.ds(pl.multiple_of(owner * piece_k + hv * half_k, half_k), half_k)]

    part_h = half_h // 2

    def down_half(owner, hv, q):
        return down_all.at[
            pl.ds(pl.multiple_of(hv * half_h + q * part_h, part_h), part_h),
            pl.ds(pl.multiple_of(owner * wide, wide), wide),
        ]

    def strip(buf, z, cc, xx, tag):
        if tag[1:] == "":
            return buf.at[z, cc, xx]
        deep = share // 2
        return buf.at[z, cc, xx, int(tag[1:]) * deep : (int(tag[1:]) + 1) * deep]

    def share_on(tag, buf, i):
        z = near(i)
        piece = strip(buf, z, c, x, tag)
        send((tag, "x"), piece, piece, xpeer, z, z)
        send((tag, "s"), piece, piece, sib, z, z)

    def cross_one(tag, buf, i):
        z = near(i)
        piece = strip(buf, z, c, 1 - x, tag)
        land((tag, "x"), piece, z)
        send((tag, "t"), piece, piece, sib, z, z)

    def tags(tag):
        return ("n0", "n1") if tag == "n" else (tag,)

    def cross(tag, buf, i):
        for one in tags(tag):
            cross_one(one, buf, i)

    def land_sib(tag, buf, i):
        for one in tags(tag):
            land((one, "s"), strip(buf, near(i), 1 - c, x, one), near(i))

    def settle(tag, buf, i, both=True):
        z = near(i)
        if both:
            land_sib(tag, buf, i)
        for one in tags(tag):
            land((one, "t"), strip(buf, z, 1 - c, 1 - x, one), z)

    def make_latent(cc, xx):
        here = rows_of(xx * 2 + cc)
        lat_all[me, cc, xx, :, :rank] = normalize(lat_in[here, :], gkv[...].reshape(1, -1)).astype(bf)
        lat_all[me, cc, xx, :, rank:] = (
            spun[here, :lanes] * table[0, here, :] + spun[here, lanes:] * table[1, here, :]
        ).astype(bf)

    def make_table(tt):
        here = rows_of(tt)
        place = lax.broadcasted_iota(jnp.int32, (share, lanes), 0) + (me * rows + tt * share)
        angle = place.astype(f32) * inverse[...]
        table[0, here, :] = jnp.cos(angle)
        table[1, here, :] = jnp.sin(angle)

    make_table(t)
    got_rk.wait()
    spun[...] = lax.dot_general(
        rk_in[...], turn[...], (((0,), (0,)), ((), ())), preferred_element_type=f32
    )
    got_lat.wait()
    got_gkv.wait()
    make_latent(c, x)
    pl.semaphore_wait(barrier, n + 2)
    own = lat_all.at[me, c, x]
    for i in reversed(range(1, 3)):
        send(("l", "z"), own, own, {"sp": near(i)}, near(i), me)
    got_op.wait()
    send("os", op_chip.at[c], op_chip.at[c], sib)
    for cc, xx in ((1 - c, x), (c, 1 - x), (1 - c, 1 - x)):
        make_table(xx * 2 + cc)
        make_latent(cc, xx)
    got_perm.wait()
    got_wq.wait()
    wide_q = jnp.dot(wq_in[...], perm_in[...], preferred_element_type=f32).astype(bf)
    got_q.wait()
    got_gq.wait()
    query_norm = normalize(q_in[...], gq[...].reshape(1, -1)).astype(bf)
    spread = jnp.dot(query_norm, wide_q, preferred_element_type=f32)
    first = heads * unit
    spin = (
        spread[:, first : first + lanes] * table[0] + spread[:, first + lanes : first + 2 * lanes] * table[1]
    )
    lane = lax.broadcasted_iota(jnp.int32, (rows, lanes), 1)
    for h in range(heads):
        q_all[h, :, :unit] = spread[:, h * unit : (h + 1) * unit].astype(bf)
        keep = (lane >= h * QUERY_KEY_ROTARY) & (lane < (h + 1) * QUERY_KEY_ROTARY)
        q_all[h, :, unit:] = jnp.where(keep, spin, 0.0).astype(bf)

    def hand_on(i):
        piece = lat_all.at[near(i), c, x]
        send(("l", "r"), piece, piece, {"sp": partner}, near(i), near(i), inner, ("l", "z"))

    land(("l", "z"), lat_all.at[near(1), c, x], near(1))
    share_on("l", lat_all, 1)
    land(("l", "z"), lat_all.at[near(2), c, x], near(2))
    hand_on(2)
    share_on("l", lat_all, 2)
    land(("l", "z"), lat_all.at[near(3), c, x], near(3))
    hand_on(3)
    share_on("l", lat_all, 3)
    def send_up(i, when):
        send(
            "up",
            up.at[
                pl.ds(pl.multiple_of(g * half_k, half_k), half_k),
                pl.ds(pl.multiple_of(near(i) * hid, hid), hid),
            ],
            up_half(me, g),
            {"sp": near(i)},
            near(i),
            me,
            when,
        )

    send_up(2, inner)
    send_up(1, outer)
    got_wkv.wait()
    for i in range(1, n):
        cross("l", lat_all, i)
    send_up(3, None)
    send_up(2, outer)
    send_up(1, inner)
    for i in range(1, n):
        settle("l", lat_all, i)
    for j in range(n):
        made = jnp.dot(
            lat_all[j, :, :, :, :rank].reshape(rows, rank), wkv_in[...], preferred_element_type=f32
        ).astype(bf)
        rope = lat_all[j, :, :, :, rank:].reshape(rows, lanes)
        for h in range(heads):
            kv_all[h, j * rows : (j + 1) * rows, :unit] = made[:, h * unit : (h + 1) * unit]
            kv_all[h, j * rows : (j + 1) * rows, unit:] = rope

    contract = (((1,), (1,)), ((), ()))
    low = lax.broadcasted_iota(jnp.int32, (rows, unit), 1) < vh

    def attend(h):
        scores = lax.dot_general(q_all[h], kv_all[h], contract, preferred_element_type=f32)
        scores = scores * scale_factor
        expo = jnp.exp(scores - jnp.max(scores, axis=-1, keepdims=True))
        total = jnp.sum(expo, axis=-1, keepdims=True)
        mix = jnp.dot(expo.astype(bf), kv_all[h, :, :unit], preferred_element_type=f32)
        return mix / total

    def head_cols(cc, p):
        return pl.ds(pl.multiple_of(cc * heads * vh + p * unit, unit), unit)

    for p in range(heads // 2):
        left, right = attend(2 * p), attend(2 * p + 1)
        pair = jnp.where(low, pltpu.roll(left, vh, 1), right)
        mixed[p] = pair.astype(bf)
        for xx in range(2):
            send(
                ("m", p, xx), mixed.at[p, rows_of(xx * 2 + 1 - c)], mixed_in.at[xx, :, head_cols(c, p)], sib
            )
            mixed_in[xx, :, head_cols(c, p)] = mixed[p, rows_of(xx * 2 + c), :]

    land("os", op_chip.at[1 - c])
    for p in range(heads // 2):
        for xx in range(2):
            land(("m", p, xx), mixed_in.at[xx, :, head_cols(1 - c, p)])

    tiles = width // wide
    chip_heads = 2 * heads * vh

    def project(xx, j):
        return jnp.dot(
            mixed_in[xx],
            op_chip[:, :, j * wide : (j + 1) * wide].reshape(chip_heads, wide),
            preferred_element_type=f32,
        )

    for j in range(tiles):
        branch_out[j] = project(1 - x, j).astype(bf)
        send(("b", j), branch_out.at[j], branch_in.at[j], xpeer)
    got_hid.wait()
    for j in range(tiles):
        kept = project(x, j)
        land(("b", j), branch_in.at[j])
        cols = slice(j * wide, (j + 1) * wide)
        middle[:, cols] = (hid_in[:, cols].astype(f32) + (kept + branch_in[j].astype(f32))).astype(bf)
    got_gain.wait()
    norm_all[me, c, x] = normalize(middle[...], gain[...].reshape(1, -1)).astype(bf)

    def pass_on(i, to, when, one):
        z = near(i)
        piece = strip(norm_all, z, c, x, one)
        send((one, "z"), piece, piece, {"sp": to}, z, z, when)

    def send_down(i, when):
        for q in range(2):
            send(
                ("dn", q),
                down.at[pl.ds(pl.multiple_of(near(i) * hid + g * half_h + q * part_h, part_h), part_h)],
                down_half(me, g, q),
                {"sp": near(i)},
                near(i),
                me,
                when,
            )

    for one in tags("n"):
        own = strip(norm_all, me, c, x, one)
        send((one, "z"), own, own, {"sp": partner}, me, me)
        send((one, "c"), own, own, {"sp": far_gate}, None, me, inner, (one, "z"))
        share_on(one, norm_all, 0)
    send_down(1, outer)
    def forward_up(i, when):
        piece = up_half(near(i), g)
        if when is None:
            land("up", piece, near(i))
        else:
            pl.when(when)(lambda: land("up", piece, near(i)))
        send("uy", piece, piece, ypeer, near(i), near(i), when)

    forward_up(1, None)
    forward_up(2, None)
    forward_up(3, None)

    def raise_block(i):
        z = near(i)
        upward = jnp.dot(norm_all[z].reshape(rows, width), up_all[...], preferred_element_type=f32)
        act[z] = jnp.square(jnp.maximum(upward, 0.0)).astype(bf)

    def relay(i, to):
        for one in tags("n"):
            land((one, "z"), strip(norm_all, near(i), c, x, one), near(i))
            pass_on(i, to, inner, one)
            share_on(one, norm_all, i)

    def forward(i, when):
        j = near(i)
        for q in range(2):
            piece = down_half(j, g, q)
            if when is None:
                land(("dn", q), piece, j)
            else:
                pl.when(when)(lambda: land(("dn", q), piece, j))
            send(("dy", q), piece, piece, ypeer, j, j, when)

    relay(1, far_gate)
    cross("n", norm_all, 0)
    relay(2, partner)
    cross("n", norm_all, 1)
    relay(3, partner)
    land_sib("n", norm_all, 3)
    send_down(2, inner)
    send_down(3, outer)
    send_down(2, outer)
    cross("n", norm_all, 2)
    send_down(3, inner)
    send_down(1, inner)
    for i in range(1, n):
        land("uy", up_half(near(i), 1 - g), near(i))
    got_up.wait()
    settle("n", norm_all, 0)
    raise_block(0)
    cross("n", norm_all, 3)
    settle("n", norm_all, 1)
    raise_block(1)
    settle("n", norm_all, 2)
    raise_block(2)
    forward(1, inner)
    settle("n", norm_all, 3, False)
    raise_block(3)

    def block(j):
        return pl.ds(pl.multiple_of(j * wide, wide), wide)

    def arrive(i):
        if i:
            for q in range(2):
                land(("dy", q), down_half(near(i), 1 - g, q), near(i))
        else:
            got_down.wait()

    def lower(i):
        j = near(i)

        @pl.loop(0, n)
        def _(d):
            made = jnp.dot(act[d], down_all[:, block(j)], preferred_element_type=f32)
            made = made.astype(bf).reshape(2, 2, share, wide)
            part[j, 0, d] = made[0]
            part[j, 1, d] = made[1]

        send("f1", part.at[j, 1 - c], rf1.at[j], sib, j, j)

    def fold_core(i):
        j = near(i)
        land("f1", rf1.at[j], j)
        c2[j] = (part[j, c, :, 1 - x].astype(f32) + rf1[j, :, 1 - x].astype(f32)).astype(bf)
        send("f2", c2.at[j], rf2.at[j], xpeer, j, j)

    def fold_x(i):
        j = near(i)
        land("f2", rf2.at[j], j)
        c3[j] = (
            part[j, c, :, x].astype(f32) + rf1[j, :, x].astype(f32) + rf2[j].astype(f32)
        ).astype(bf)
        send("pe", c3.at[j, far_edge], near_in.at[j, 2], {"sp": partner}, j, j, outer)
        send("pg", c3.at[j, far_gate], near_in.at[j, 1], {"sp": partner}, j, j, outer)
        send("p", c3.at[j, partner], near_in.at[j, 0], {"sp": partner}, j, j)

    def fold_side(i):
        j = near(i)

        @pl.when(inner)
        def _():
            land("pe", near_in.at[j, 2], j)
            cross_out[j, 1] = (c3[j, far_edge].astype(f32) + near_in[j, 2].astype(f32)).astype(bf)

        send("q1", cross_out.at[j, 1], cross_in.at[j], {"sp": far_edge}, j, j, inner, "q0")

        @pl.when(inner)
        def _():
            land("pg", near_in.at[j, 1], j)
            cross_out[j, 0] = (c3[j, far_gate].astype(f32) + near_in[j, 1].astype(f32)).astype(bf)

        send("q0", cross_out.at[j, 0], cross_in.at[j], {"sp": far_gate}, j, j, inner)

    def finish(i):
        j = near(i)
        land("p", near_in.at[j, 0], j)
        land("q0", cross_in.at[j], j)
        feed = c3[j, me].astype(f32) + near_in[j, 0].astype(f32) + cross_in[j].astype(f32)
        out[:, block(j)] = (middle[:, block(j)].astype(f32) + feed).astype(bf)

    arrive(0)
    lower(0)
    fold_core(0)
    forward(1, outer)
    forward(2, None)
    arrive(1)
    lower(1)
    fold_core(1)
    forward(3, None)
    fold_x(0)
    arrive(2)
    lower(2)
    fold_core(2)
    fold_x(1)
    arrive(3)
    lower(3)
    fold_core(3)
    fold_x(2)
    fold_side(1)
    fold_side(0)
    fold_x(3)
    fold_side(2)
    fold_side(3)
    for i in range(n):
        finish(i)
    for copy, when in sent:
        if when is None:
            copy.wait_send()
        else:
            pl.when(when)(copy.wait_send)


def spread_columns(heads):
    head = QUERY_KEY_PLAIN + QUERY_KEY_ROTARY
    half = QUERY_KEY_ROTARY // 2
    unit = QUERY_KEY_PLAIN + VALUE_HEAD_SIZE
    lanes = heads * QUERY_KEY_ROTARY
    perm = np.zeros((heads * head, heads * unit + 2 * lanes), np.float32)
    turn = np.zeros((QUERY_KEY_ROTARY, 2 * lanes), np.float32)
    for h in range(heads):
        for r in range(QUERY_KEY_PLAIN):
            perm[h * head + r, h * unit + r] = 1.0
        for r in range(QUERY_KEY_ROTARY):
            col = h * QUERY_KEY_ROTARY + r
            other, sign = (r + half, -1.0) if r < half else (r - half, 1.0)
            turn[r, col] = 1.0
            turn[other, lanes + col] = sign
            perm[h * head + QUERY_KEY_PLAIN + r, heads * unit + col] = 1.0
            perm[h * head + QUERY_KEY_PLAIN + other, heads * unit + lanes + col] = sign
    return jnp.asarray(perm, jnp.bfloat16), jnp.asarray(turn, jnp.bfloat16)


def run_layer(
    hidden_in, query_latent_rows, key_value_latent, rotary_key, query_norm_gain, key_value_gain,
    query_up_weight, key_value_up_weight, out_proj, feed_gain, feed_up, feed_down, position,
):
    n = lax.axis_size("sp")
    rows, width = hidden_in.shape
    heads = query_up_weight.shape[1] // (QUERY_KEY_PLAIN + QUERY_KEY_ROTARY)
    share = rows // lax.axis_size("tp")
    hid = feed_up.shape[1] // n
    unit = QUERY_KEY_PLAIN + VALUE_HEAD_SIZE
    lanes = heads * QUERY_KEY_ROTARY
    rank = key_value_latent.shape[1]
    bf = jnp.bfloat16
    half = QUERY_KEY_ROTARY // 2
    inverse = 10000.0 ** (-np.arange(half, dtype=np.float32) * 2.0 / QUERY_KEY_ROTARY)
    inverse = jnp.asarray(np.tile(inverse, lanes // half)[None, :], jnp.float32)
    perm, turn = spread_columns(heads)
    vmem = pl.BlockSpec(memory_space=pltpu.VMEM)
    anywhere = pl.BlockSpec(memory_space=pl.ANY)
    wide = width // n
    copies = 29 * n
    block = (share, width)
    return pl.pallas_call(
        lambda *refs: layer_kernel(heads, *refs),
        out_shape=pltpu.VMEM(block, bf),
        in_specs=[vmem] * 2 + [anywhere] * 13,
        out_specs=vmem,
        scratch_shapes=[
            pltpu.VMEM((2, rows, lanes), jnp.float32),
            pltpu.VMEM((rows, 2 * lanes), jnp.float32),
            pltpu.VMEM(query_norm_gain.shape, jnp.float32),
            pltpu.VMEM(key_value_gain.shape, jnp.float32),
            pltpu.VMEM(feed_gain.shape, jnp.float32),
            pltpu.VMEM(key_value_latent.shape, bf),
            pltpu.VMEM(rotary_key.T.shape, bf),
            pltpu.VMEM(query_latent_rows.shape, bf),
            pltpu.VMEM(query_up_weight.shape, bf),
            pltpu.VMEM(key_value_up_weight.shape, bf),
            pltpu.VMEM(perm.shape, bf),
            pltpu.VMEM(block, bf),
            pltpu.VMEM((n, 2, 2, share, rank + lanes), bf),
            pltpu.VMEM((heads, n * rows, unit + lanes), bf),
            pltpu.VMEM((heads, rows, unit + lanes), bf),
            pltpu.VMEM((2, *out_proj.shape), bf),
            pltpu.VMEM((heads // 2, rows, unit), bf),
            pltpu.VMEM((2, share, out_proj.shape[0] * 2), bf),
            pltpu.VMEM((n, share, wide), bf),
            pltpu.VMEM((n, share, wide), bf),
            pltpu.VMEM((feed_up.shape[0] * n, hid), bf),
            pltpu.VMEM((hid, width), bf),
            pltpu.VMEM(block, bf),
            pltpu.VMEM((n, 2, 2, *block), bf),
            pltpu.VMEM((n, rows, hid), bf),
            pltpu.VMEM((n, 2, n, 2, share, wide), bf),
            pltpu.VMEM((n, n, 2, share, wide), bf),
            pltpu.VMEM((n, n, share, wide), bf),
            pltpu.VMEM((n, n, share, wide), bf),
            pltpu.VMEM((n, n, share, wide), bf),
            pltpu.VMEM((n, 3, share, wide), bf),
            pltpu.VMEM((n, 2, share, wide), bf),
            pltpu.VMEM((n, share, wide), bf),
            pltpu.SemaphoreType.DMA((copies,)),
            pltpu.SemaphoreType.DMA((copies,)),
            pltpu.SemaphoreType.DMA((16,)),
        ],
        compiler_params=pltpu.CompilerParams(
            collective_id=0, has_side_effects=True, vmem_limit_bytes=60 * 1024 * 1024
        ),
    )(
        inverse, turn, key_value_latent, rotary_key.T, query_latent_rows, query_norm_gain,
        key_value_gain, feed_gain, perm, query_up_weight, key_value_up_weight, hidden_in, out_proj,
        feed_up, feed_down,
    )


def fits_kernel(tokens, query_up_weight, feed_up):
    n = lax.axis_size("sp")
    hid = feed_up.shape[1] // n
    heads = query_up_weight.shape[1] // (QUERY_KEY_PLAIN + QUERY_KEY_ROTARY)
    return (
        lax.axis_size("grp") == 2
        and lax.axis_size("tp") == 4
        and n == 4
        and tokens * n <= 1024
        and tokens % 64 == 0
        and hid % 128 == 0
        and hid <= 512
        and heads * QUERY_KEY_ROTARY == 128
    )


def on_device(
    hidden_in,
    query_latent_rows,
    key_value_latent,
    rotary_key,
    query_norm_gain,
    key_value_gain,
    query_up_weight,
    key_value_up_weight,
    out_proj,
    feed_gain,
    feed_up,
    feed_down,
):
    tokens_here = hidden_in.shape[0]
    heads_here = query_up_weight.shape[1] // (QUERY_KEY_PLAIN + QUERY_KEY_ROTARY)
    position = (lax.axis_index("sp") * tokens_here + jnp.arange(tokens_here)).astype(jnp.float32)
    if fits_kernel(tokens_here, query_up_weight, feed_up):
        return run_layer(
            hidden_in, query_latent_rows, key_value_latent, rotary_key, query_norm_gain,
            key_value_gain, query_up_weight, key_value_up_weight, out_proj, feed_gain, feed_up,
            feed_down, position,
        )
    scale_factor = (QUERY_KEY_PLAIN + QUERY_KEY_ROTARY) ** (-0.5)
    query_norm = normalize(query_latent_rows, query_norm_gain).astype(jnp.bfloat16)
    queries = jnp.dot(query_norm, query_up_weight, preferred_element_type=jnp.float32).reshape(
        tokens_here, heads_here, QUERY_KEY_PLAIN + QUERY_KEY_ROTARY
    )
    queries = jnp.concatenate(
        [queries[..., :QUERY_KEY_PLAIN], rotate(queries[..., QUERY_KEY_PLAIN:], position)], axis=-1
    ).astype(jnp.bfloat16)
    query_plain = queries[..., :QUERY_KEY_PLAIN]
    query_turned = queries[..., QUERY_KEY_PLAIN:]
    latent = normalize(key_value_latent, key_value_gain).astype(jnp.bfloat16)
    key_rope = rotate(rotary_key.astype(jnp.float32), position).astype(jnp.bfloat16)

    def attend_block(carry, key_plain, value_rows, rope_rows):
        row_max, denom, accum = carry
        scores = jnp.einsum(
            "qhd,khd->hqk", query_plain, key_plain, preferred_element_type=jnp.float32
        )
        scores = scores + jnp.einsum(
            "qhd,kd->hqk", query_turned, rope_rows, preferred_element_type=jnp.float32
        )
        scores = scores * scale_factor
        new_max = jnp.maximum(row_max, jnp.max(scores, axis=-1))
        expo = jnp.exp(scores - new_max[:, :, None])
        factor = jnp.exp(row_max - new_max)
        denom = denom * factor + jnp.sum(expo, axis=-1)
        update = jnp.einsum(
            "hqk,khd->qhd",
            expo.astype(jnp.bfloat16),
            value_rows,
            preferred_element_type=jnp.float32,
        )
        accum = accum * jnp.transpose(factor)[:, :, None] + update
        return (new_max, denom, accum)

    start_carry = (
        jnp.full((heads_here, tokens_here), -1e30, jnp.float32),
        jnp.zeros((heads_here, tokens_here), jnp.float32),
        jnp.zeros((tokens_here, heads_here, VALUE_HEAD_SIZE), jnp.float32),
    )
    own_keys = jnp.dot(latent, key_value_up_weight, preferred_element_type=jnp.float32).astype(
        jnp.bfloat16
    )
    pieces = (
        lax.all_gather(own_keys, "sp", axis=0, tiled=True),
        lax.all_gather(key_rope, "sp", axis=0, tiled=True),
    )
    rows_in = pieces[0].shape[0]
    block = math.gcd(rows_in, 1024)

    def step_block(index, inner):
        first = index * block
        bulk = lax.dynamic_slice_in_dim(pieces[0], first, block, 0)
        rope_rows = lax.dynamic_slice_in_dim(pieces[1], first, block, 0)
        bulk = bulk.reshape(block, heads_here, QUERY_KEY_PLAIN + VALUE_HEAD_SIZE)
        return attend_block(
            inner, bulk[..., :QUERY_KEY_PLAIN], bulk[..., QUERY_KEY_PLAIN:], rope_rows
        )

    final_carry = lax.fori_loop(0, rows_in // block, step_block, start_carry)
    denom = final_carry[1]
    accum = final_carry[2]
    mixed = (
        (accum / jnp.transpose(denom)[:, :, None])
        .astype(jnp.bfloat16)
        .reshape(tokens_here, heads_here * VALUE_HEAD_SIZE)
    )
    up_own = lax.all_to_all(feed_up, "sp", split_axis=1, concat_axis=0, tiled=True)
    down_own = lax.all_to_all(feed_down, "sp", split_axis=0, concat_axis=1, tiled=True)
    share = tokens_here // lax.axis_size("tp")
    lead = lax.axis_index("tp") * share
    branch = lax.psum_scatter(
        jnp.dot(mixed, out_proj, preferred_element_type=jnp.float32).astype(jnp.bfloat16),
        "tp",
        scatter_dimension=0,
        tiled=True,
    ).astype(jnp.float32)
    hidden_own = lax.dynamic_slice_in_dim(hidden_in, lead, share, 0)
    middle_own = (hidden_own.astype(jnp.float32) + branch).astype(jnp.bfloat16)
    normed_own = normalize(middle_own, feed_gain).astype(jnp.bfloat16)
    normed = lax.all_gather(normed_own, ("sp", "tp"), axis=0, tiled=True)
    upward = jnp.dot(normed, up_own, preferred_element_type=jnp.float32)
    activated = jnp.square(jax.nn.relu(upward)).astype(jnp.bfloat16)
    partial_sum = jnp.dot(activated, down_own, preferred_element_type=jnp.float32)
    feed = lax.psum_scatter(
        partial_sum.astype(jnp.bfloat16), ("sp", "tp"), scatter_dimension=0, tiled=True
    ).astype(jnp.float32)
    return (middle_own.astype(jnp.float32) + feed).astype(jnp.bfloat16)


def solution(mesh):
    return jax.shard_map(
        on_device,
        mesh=mesh,
        in_specs=(
            P(("grp", "sp"), None),
            P(("grp", "sp"), None),
            P(("grp", "sp"), None),
            P(("grp", "sp"), None),
            P(),
            P(),
            P(None, "tp"),
            P(None, "tp"),
            P("tp", None),
            P(),
            P("sp", "tp"),
            P("tp", "sp"),
        ),
        out_specs=P(("grp", "sp", "tp"), None),
        check_vma=False,
    )
```
